32 devices in a mesh: rep: 2 (over y), fs: 4 (over z), tp: 4 (over x, core).
Axes of the slice: x: 2, y: 2, z: 4, core: 2. Of those that a mesh axis runs over, the one named last changes fastest.
Arguments:
- tokens: bfloat16 [4096, 2048], P(('rep', 'fs')), may hold values from -6 to 6
- norm_gain: float32 [2048], replicated, may hold values from 0.1 to 1.9
- gate_weight: bfloat16 [2048, 5632], P('fs', 'tp'), may hold values from -0.125 to 0.125
- up_weight: bfloat16 [2048, 5632], P('fs', 'tp'), may hold values from -0.125 to 0.125
- down_weight: bfloat16 [5632, 2048], P('tp', 'fs'), may hold values from -0.078125 to 0.078125
Outputs:
- branch_out: bfloat16 [4096, 2048], P(('rep', 'fs'))
The draws below stay inside these ranges and needn't reach their ends.
All inputs are finite; a program needn't handle non-finite values.
Results may differ from the reference program's by a relative error of at most 0.014.
Values may be sent and summed in bfloat16 or wider, within the bound.
A program may use at most 64 MiB of HBM per device.

```python
import jax
import jax.numpy as jnp
from jax import lax

D = 2048
FF = 5632
TOKENS = 4096
N_TP = 4


def steps_of(key, shape, cuts, low, top_value):
    def one(axis_at, blocks):
        steps = jax.random.uniform(jax.random.fold_in(jax.random.fold_in(key, 6), axis_at), (blocks,), jnp.float32, low / len(cuts), top_value / len(cuts))
        return jnp.repeat(jnp.exp(steps), shape[axis_at] // blocks).reshape((-1,) + (1,) * (len(shape) - axis_at - 1))

    level = one(*cuts[0])
    for cut in cuts[1:]:
        level = level * one(*cut)
    return level


def gaussian(rng, shape, scale, most, split=(), kind=jnp.bfloat16):
    drawn = scale * jax.random.normal(rng, shape, jnp.float32)
    if split:
        drawn = drawn * steps_of(rng, shape, split, -0.22, 0.18)
    return jnp.clip(drawn, -most, most).astype(kind)


def setup_inputs(seed: int = 0) -> dict:
    streams_of = jax.random.split(jax.random.key(seed), 6)
    return {
        "tokens": gaussian(streams_of[0], (TOKENS, D), 1.0, 6.0, ((0, 8),)),
        "norm_gain": jnp.clip(1.0 + 0.18 * jax.random.normal(streams_of[1], (D,), jnp.float32), 0.1, 1.9),
        "gate_weight": gaussian(streams_of[2], (D, FF), D ** -0.5, 0.125, ((0, 4), (1, 4))),
        "up_weight": gaussian(streams_of[3], (D, FF), D ** -0.5, 0.125, ((0, 4), (1, 4))),
        "down_weight": gaussian(streams_of[4], (FF, D), FF ** -0.5, 0.078125, ((0, 4), (1, 4))),
    }


def reference(tokens, norm_gain, gate_weight, up_weight, down_weight):
    wide_tok = tokens.astype(jnp.float32)
    scale = jax.lax.rsqrt(lax.optimization_barrier(jnp.mean(wide_tok * wide_tok, axis=-1, keepdims=True)) + 1e-06)
    normed = (wide_tok * scale * norm_gain).astype(jnp.bfloat16)
    gate = jnp.dot(normed, gate_weight, preferred_element_type=jnp.float32)
    up = jnp.dot(normed, up_weight, preferred_element_type=jnp.float32)
    hidden = (jax.nn.silu(gate) * up).astype(jnp.bfloat16)
    width = FF // N_TP
    total = jnp.zeros((hidden.shape[0], D), jnp.float32)
    for block in range(N_TP):
        partial_value = jnp.dot(hidden[:, block * width:(block + 1) * width], down_weight[block * width:(block + 1) * width], preferred_element_type=jnp.float32).astype(jnp.bfloat16)
        total = total + partial_value.astype(jnp.float32)
    return total.astype(jnp.bfloat16)
```

```python
import functools

import jax
import jax.numpy as jnp
from jax import lax
from jax.experimental import pallas as pl
from jax.experimental.pallas import tpu as pltpu
from jax.sharding import PartitionSpec as P

MESH = pl.DeviceIdType.MESH
F32 = jnp.float32
BF16 = jnp.bfloat16


def plain(tokens, norm_gain, gate_weight, up_weight, down_weight):
    wide_tok = tokens.astype(F32)
    scale = lax.rsqrt(jnp.mean(wide_tok * wide_tok, axis=-1, keepdims=True) + 1e-06)
    normed = (wide_tok * scale * norm_gain).astype(BF16)
    gate = jnp.dot(normed, lax.all_gather(gate_weight, "fs", axis=0, tiled=True), preferred_element_type=F32)
    up = jnp.dot(normed, lax.all_gather(up_weight, "fs", axis=0, tiled=True), preferred_element_type=F32)
    hidden = (jax.nn.silu(gate) * up).astype(BF16)
    down = lax.all_gather(down_weight, "fs", axis=1, tiled=True)
    partial_value = jnp.dot(hidden, down, preferred_element_type=F32)
    return lax.psum(partial_value.astype(BF16), "tp")


CUTS = ((2, 2), (2, 1, 1))
KINDS = (1, 0, 0, 1)
MOST_CUTS = 3
SUBS = 2
MID = 128


def spans_of(which, width):
    spans, at = [], 0
    for part in CUTS[which]:
        spans.append((at, part * width // 4))
        at += part * width // 4
    return spans


def plan(width):
    block, hop, start = 15.4, 2.2, 67.2
    free = {"x": 0.0, "z": 0.0, "weights": 71.7, "core": 74.0}
    todo = [(72.0, "last", 0, 0)]

    def book(link, when, size):
        free[link] = max(free[link], when) + size
        return free[link]

    for s in range(4):
        for i, (at, size) in enumerate(spans_of(KINDS[s], width)):
            share = block * size / width
            ready = 70.0
            if s == 1:
                out = 64.0 + block * (at + size) / width / 2 + hop
                todo.append((out, "end", s, i))
                ready = out + share / 2 + hop
            if s >= 2:
                begin = start + (s - 2) * block + block * at / width
                far, near = begin + 0.55 * share + hop, begin + share + hop
                out = book("weights", far, share / 2) + hop
                todo += [(far, "far", s, i), (near, "near", s, i), (out, "end", s, i)]
                ready = max(near, out) + share / 2 + hop
            done = book("core", ready, 1.2 * size / 256 + 0.2)
            todo.append((done, "use", s, i))
    uses = [(when, s, i) for when, kind, s, i in todo if kind == "use"]
    pend = [(when + 1.8, 1, s, i) for when, s, i in uses]
    while pend:
        pend.sort()
        when, stage, s, i = pend.pop(0)
        todo.append((when, stage, s, i))
        size = spans_of(KINDS[s], width)[i][1]
        half = block * size / width * 5.5 / 15.4
        path = ROUTES[direct(s, i)]
        if stage <= len(path):
            link, scale = path[stage - 1]
            after = when + 1.5 if link == "core" else book(link, when, half * scale) + hop
            pend.append((after, stage + 1, s, i))
    todo.sort(key=lambda item: item[0])
    return [item[1:] for item in todo]


ROUTES = (
    (("x", 1.0), ("z", 0.8), ("x", 0.5), ("core", 0.0)),
    (("z", 1.0), ("x", 1.0), ("core", 0.0)),
)


def direct(s, i):
    return int(s == 3 or s == 1)


def kernel(
    n, tok_ref, gain_ref, wg_ref, wu_ref, wd_ref, out_ref,
    tokv, tokp, normed, bw, bd, acc, hidden, part, r1, sbuf, rz, sx, r2, outv,
    loc_sem, zsend, zrecv, dsend, drecv, ysend, yrecv, vsend, vrecv, tsend, trecv,
    psend, precv, wsend, wrecv, xsend, xrecv, asend, arecv, qsend, qrecv, osem,
):
    z = lax.axis_index("fs")
    y = lax.axis_index("rep")
    t = lax.axis_index("tp")
    c = lax.rem(t, 2)
    tokens, width = tok_ref.shape
    depth, units = wg_ref.shape
    cols = wd_ref.shape[1]
    spans = tuple(spans_of(which, cols) for which in (0, 1))
    half_k, half_t, quarter = depth // 2, tokens // 2, tokens // 4
    sub_k = half_k // SUBS
    most = (units - MID) // 2
    e = lax.rem(z, 2)
    hi = z // 2
    inner = e != hi
    near = z + 1 - 2 * e
    third = 2 - hi
    fourth = 3 - 3 * hi
    pair = {"fs": near}
    has_mid = e == c
    mine = pl.multiple_of(e * (most + MID), MID)
    first_unit = pl.multiple_of(e * jnp.where(has_mid, most, most + MID), MID)
    mate = {"tp": t + 1 - 2 * c}
    across = {"tp": lax.rem(t + 2, 4)}
    row = t // 2
    first_block, second_block = 3 * hi, 1 + hi
    peer = {"rep": 1 - y}

    barrier = pltpu.get_barrier_semaphore()

    around = ({"fs": lax.rem(z + 1, n)}, {"fs": lax.rem(z + n - 1, n)})
    others = tuple({"tp": lax.rem(t + d, 4)} for d in (1, 2, 3))
    for one in around + others + (peer,):
        pl.semaphore_signal(barrier, 1, device_id=one, device_id_type=MESH)
    tok_copy = pltpu.make_async_copy(tok_ref, tokv, loc_sem.at[3])
    tok_copy.start()
    pl.semaphore_wait(barrier, 6)

    def token_move(quart, to, sem, first):
        at = pl.ds(pl.multiple_of(quart * quarter, quarter), quarter)
        return pltpu.make_async_remote_copy(
            src_ref=(tok_ref if first else tokp).at[at],
            dst_ref=tokp.at[at],
            send_sem=tsend.at[sem],
            recv_sem=trecv.at[quart],
            device_id=to,
            device_id_type=MESH,
        )

    def start_of(r, way):
        if r == 1:
            return most, MID
        side = way if r == 0 else 1 - way
        return pl.multiple_of(side * (most + MID), MID), most

    def side_of(r, way):
        return c if r == 1 else (way if r == 0 else 1 - way)

    def passes(r, way):
        q = side_of(r, way)
        return jnp.logical_or(
            jnp.logical_and(way == 0, z > q), jnp.logical_and(way == 1, z < n - 2 + q))

    def arrives(r, way):
        q = side_of(r, way)
        return jnp.logical_or(
            jnp.logical_and(way == 0, z >= q), jnp.logical_and(way == 1, z < n - 1 + q))

    def pieces(r):
        return range(1 if r == 1 else SUBS)

    def rows_of(r, s, who):
        if r == 1:
            return pl.ds(pl.multiple_of(who * half_k, half_k), half_k)
        return pl.ds(pl.multiple_of(who * half_k + s * sub_k, sub_k), sub_k)

    def along(u, blk, r, s, way, own=None):
        start, size = start_of(r, way)
        at = (rows_of(r, s, y), pl.ds(start, size))
        return pltpu.make_async_remote_copy(
            src_ref=bw.at[(u, blk) + at] if own is None else own.at[at],
            dst_ref=bw.at[(u, blk) + at],
            send_sem=zsend.at[u, blk, r, s, way],
            recv_sem=zrecv.at[u, blk, r, s],
            device_id={"fs": z - 1 + 2 * way},
            device_id_type=MESH,
        )

    def swap(u, blk, i, s, who):
        start, size = ((mine, most), (most, MID))[i]
        place = bw.at[u, blk, rows_of(i, s, who), pl.ds(start, size)]
        return pltpu.make_async_remote_copy(
            src_ref=place,
            dst_ref=place,
            send_sem=ysend.at[u, blk, i, s],
            recv_sem=yrecv.at[u, blk, i, s],
            device_id=peer,
            device_id_type=MESH,
        )

    def d_rows(start, size, who):
        return pl.ds(pl.multiple_of(start + who * (size // 2), 64), size // 2)

    def d_along(blk, i, span, r, way, own=False):
        start, size = start_of(r, way)
        at = (d_rows(start, size, y), pl.ds(*span))
        return pltpu.make_async_remote_copy(
            src_ref=wd_ref.at[at] if own else bd.at[(blk,) + at],
            dst_ref=bd.at[(blk,) + at],
            send_sem=dsend.at[blk, i, r, way],
            recv_sem=drecv.at[blk, i, r],
            device_id={"fs": z - 1 + 2 * way},
            device_id_type=MESH,
        )

    def d_swap(blk, i, span, p, who):
        start, size = ((mine, most), (most, MID))[p]
        place = bd.at[blk, d_rows(start, size, who), pl.ds(*span)]
        return pltpu.make_async_remote_copy(
            src_ref=place,
            dst_ref=place,
            send_sem=vsend.at[blk, i, p],
            recv_sem=vrecv.at[blk, i, p],
            device_id=peer,
            device_id_type=MESH,
        )

    def own_pieces(way, body):
        for u, own in ((0, wg_ref), (1, wu_ref)):
            for r in range(3):
                @pl.when(passes(r, way))
                def _():
                    for s in pieces(r):
                        body(along(u, z, r, s, way, own))

    def own_d_pieces(which, way, body):
        for i, span in enumerate(spans[which]):
            for r in range(3):
                pl.when(passes(r, way))(lambda: body(d_along(z, i, span, r, way, True)))

    go = lambda copy: copy.start()
    ZERO, ONE = jnp.int32(0), jnp.int32(1)
    inward, outward = 1 - hi, hi
    @pl.when(inner)
    def _():
        own_pieces(inward, go)
        token_move(t, pair, 0, True).start()
        own_pieces(outward, go)

    @pl.when(jnp.logical_not(inner))
    def _():
        token_move(t, pair, 0, True).start()
        own_pieces(inward, go)
        own_d_pieces(1, inward, go)

    locals_ = [
        pltpu.make_async_copy(wg_ref, bw.at[0, z], loc_sem.at[0]),
        pltpu.make_async_copy(wu_ref, bw.at[1, z], loc_sem.at[1]),
        pltpu.make_async_copy(wd_ref, bd.at[z], loc_sem.at[2]),
    ]
    for copy in locals_:
        copy.start()

    step = 64

    def norm(src, base):
        @pl.loop(0, tokens // step)
        def _(i):
            at = pl.ds(pl.multiple_of(i * step, step), step)
            to = pl.ds(pl.multiple_of(base + i * step, step), step)
            wide = src[at, :].astype(F32)
            scale = lax.rsqrt(jnp.mean(wide * wide, axis=-1, keepdims=True) + 1e-06)
            normed[to, :] = (wide * scale * gain_ref[...]).astype(BF16)

    def by_size(body):
        pl.when(has_mid)(lambda: body(most + MID))
        pl.when(jnp.logical_not(has_mid))(lambda: body(most))

    def add_dot(u, blk, first=False, last=False):
        def piece(size):
            to = pl.ds(0, size)

            @pl.loop(0, 4)
            def _(i):
                at = pl.ds(pl.multiple_of(i * half_t, half_t), half_t)
                left = normed[at, pl.ds(pl.multiple_of(blk * depth, depth), depth)]
                value = jnp.dot(left, bw[u, blk, :, pl.ds(first_unit, size)], preferred_element_type=F32)
                if first:
                    acc[u, at, to] = value
                elif last:
                    hidden[at, to] = (acc[0, at, to] * (acc[1, at, to] + value)).astype(BF16)
                else:
                    acc[u, at, to] = acc[u, at, to] + value

        by_size(piece)

    def activate():
        def piece(size):
            to = pl.ds(0, size)

            @pl.loop(0, 2 * tokens // step)
            def _(i):
                at = pl.ds(pl.multiple_of(i * step, step), step)
                value = acc[0, at, to]
                acc[0, at, to] = value / (1.0 + jnp.exp(-value))

        by_size(piece)

    def place(blk, span, start, size):
        return (
            pl.ds(pl.multiple_of(start, size), size),
            pl.ds(pl.multiple_of(blk * cols + span[0], 128), span[1]),
        )

    def remote(src, dst, sems, at, to):
        return pltpu.make_async_remote_copy(
            src, dst, sems[0].at[at], sems[1].at[at], device_id=to, device_id_type=MESH)

    def to_mate(blk, i, span):
        return remote(part.at[blk, 1, :, :, :, pl.ds(*span)], r1.at[blk, :, :, :, pl.ds(*span)], (psend, precv), (blk, i), mate)

    def line_all(blk, i, span):
        return remote(sbuf.at[blk, 1, :, :, pl.ds(*span)], rz.at[blk, :, :, pl.ds(*span)], (wsend, wrecv), (blk, i), pair)

    def line_one(blk, i, span):
        return remote(sx.at[blk, 1, :, pl.ds(*span)], rz.at[blk, 0, :, pl.ds(*span)], (wsend, wrecv), (blk, i), pair)

    def cross_all(blk, i, span):
        return remote(sx.at[blk, :, :, pl.ds(*span)], r2.at[blk, :, :, pl.ds(*span)], (xsend, xrecv), (blk, i), across)

    def cross_one(blk, i, span):
        return remote(sbuf.at[blk, :, 1 - row, :, pl.ds(*span)], r2.at[blk, :, :, pl.ds(*span)], (xsend, xrecv), (blk, i), across)

    def share(blk, i, span, who):
        at = outv.at[place(blk, span, c * half_t + who * quarter, quarter)]
        return remote(at, at, (asend, arecv), (blk, i), across)

    def give(blk, i, span, who):
        at = outv.at[place(blk, span, who * half_t, half_t)]
        return remote(at, at, (qsend, qrecv), (blk, i), mate)

    def write(blk, i, span):
        at = pl.ds(pl.multiple_of(blk * cols + span[0], 128), span[1])
        return pltpu.make_async_copy(outv.at[:, at], out_ref.at[:, at], osem.at[blk, i])

    def make_part(blk, i, span):
        def fill(size, side):
            @pl.loop(0, 2)
            def _(which):
                whose = c + side - 2 * c * side
                at = pl.ds(pl.multiple_of(which * tokens + whose * half_t, half_t), half_t)
                value = jnp.dot(
                    hidden[at, pl.ds(0, size)], bd[blk, pl.ds(first_unit, size), pl.ds(*span)],
                    preferred_element_type=F32)
                part[blk, side, which, :, :, pl.ds(*span)] = value.astype(BF16).reshape(2, quarter, span[1])

        by_size(lambda size: fill(size, 1))
        to_mate(blk, i, span).start()
        by_size(lambda size: fill(size, 0))

    def sum_mate(blk, i, span):
        to_mate(blk, i, span).wait_recv()
        at = pl.ds(*span)
        sbuf[blk, :, :, :, at] = (part[blk, 0, :, :, :, at].astype(F32) + r1[blk, :, :, :, at].astype(F32)).astype(BF16)

    def direct_1(blk, i, span):
        sum_mate(blk, i, span)
        line_all(blk, i, span).start()

    def direct_2(blk, i, span):
        line_all(blk, i, span).wait_recv()
        at = pl.ds(*span)
        sx[blk, :, :, at] = (sbuf[blk, 0, :, :, at].astype(F32) + rz[blk, :, :, at].astype(F32)).astype(BF16)
        cross_all(blk, i, span).start()

    def direct_3(blk, i, span):
        cross_all(blk, i, span).wait_recv()
        at = pl.ds(*span)
        value = (sx[blk, :, :, at].astype(F32) + r2[blk, :, :, at].astype(F32)).astype(BF16)
        outv[place(blk, span, c * half_t, half_t)] = value.reshape(half_t, span[1])
        give(blk, i, span, c).start()

    def split_1(blk, i, span):
        sum_mate(blk, i, span)
        cross_one(blk, i, span).start()

    def split_2(blk, i, span):
        cross_one(blk, i, span).wait_recv()
        at = pl.ds(*span)
        sx[blk, :, :, at] = (sbuf[blk, :, row, :, at].astype(F32) + r2[blk, :, :, at].astype(F32)).astype(BF16)
        line_one(blk, i, span).start()

    def split_3(blk, i, span):
        line_one(blk, i, span).wait_recv()
        at = pl.ds(*span)
        outv[place(blk, span, c * half_t + row * quarter, quarter)] = (
            sx[blk, 0, :, at].astype(F32) + rz[blk, 0, :, at].astype(F32)).astype(BF16)
        share(blk, i, span, row).start()

    def split_4(blk, i, span):
        share(blk, i, span, 1 - row).wait_recv()
        give(blk, i, span, c).start()

    def store(blk, i, span):
        give(blk, i, span, 1 - c).wait_recv()
        write(blk, i, span).start()

    stages = ((split_1, split_2, split_3, split_4, store), (direct_1, direct_2, direct_3, store))

    def way_of(blk):
        return jnp.where(blk < z, ONE, ZERO)

    def arrive(u, blk, rs=(0, 1, 2)):
        way = way_of(blk)
        for r in rs:
            @pl.when(arrives(r, way))
            def _():
                for s in pieces(r):
                    along(u, blk, r, s, way).wait_recv()
                    pl.when(passes(r, way))(lambda: along(u, blk, r, s, way).start())
                    pl.when(side_of(r, way) == e)(lambda: swap(u, blk, int(r == 1), s, y).start())

    def swaps(u, blk, who, body):
        for s in pieces(0):
            body(swap(u, blk, 0, s, who))

        @pl.when(has_mid)
        def _():
            for s in pieces(1):
                body(swap(u, blk, 1, s, who))

    def d_arrive(blk, i, span, rs=(0, 1, 2)):
        way = way_of(blk)
        for r in rs:
            @pl.when(arrives(r, way))
            def _():
                d_along(blk, i, span, r, way).wait_recv()
                pl.when(passes(r, way))(lambda: d_along(blk, i, span, r, way).start())
                pl.when(side_of(r, way) == e)(lambda: d_swap(blk, i, span, int(r == 1), y).start())

    def d_swaps(blk, i, span, who, body):
        body(d_swap(blk, i, span, 0, who))
        pl.when(has_mid)(lambda: body(d_swap(blk, i, span, 1, who)))

    def use(u, blk, last=False):
        swaps(u, blk, 1 - y, lambda copy: copy.wait_recv())
        add_dot(u, blk, last=last)

    zero_in = jnp.where(inner, ZERO, ONE)
    events = (
        (ZERO, jnp.where(inner, third, near)),
        (zero_in, near),
        (1 - zero_in, third),
        (ONE, jnp.where(inner, near, third)),
        (ZERO, fourth),
        (ONE, fourth),
    )

    tok_copy.wait()
    norm(tokv, 0)
    for copy in locals_:
        copy.wait()
    token_move(t, pair, 0, True).wait_recv()
    for i, one in enumerate(others):
        token_move(t, one, 1 + i, False).start()
    outer = jnp.logical_not(inner)
    arrive(*events[0])
    arrive(*events[1])
    arrive(*events[2])
    for d in (1, 2, 3):
        token_move(lax.rem(t + d, 4), mate, 0, False).wait_recv()
    norm(tokp, tokens)
    pl.when(inner)(lambda: arrive(*events[3], rs=(0,)))
    for u in (0, 1):
        add_dot(u, z, first=True)
    pl.when(inner)(lambda: arrive(*events[4], rs=(0, 1)))
    pl.when(outer)(lambda: arrive(*events[3]))
    use(*events[0])

    @pl.when(inner)
    def _():
        arrive(*events[3], rs=(1, 2))
        own_d_pieces(0, inward, go)

    use(*events[1])
    use(*events[2])
    pl.when(inner)(lambda: arrive(*events[4], rs=(2,)))
    pl.when(outer)(lambda: arrive(*events[4]))
    use(*events[3])

    @pl.when(inner)
    def _():
        d_arrive(first_block, 0, spans[1][0])
        arrive(*events[5], rs=(0,))

    use(*events[4])

    @pl.when(inner)
    def _():
        arrive(*events[5], rs=(1,))
        own_d_pieces(0, outward, go)

    activate()
    pl.when(outer)(lambda: arrive(*events[5]))

    @pl.when(inner)
    def _():
        arrive(*events[5], rs=(2,))
        for i in range(1, len(spans[1])):
            d_arrive(first_block, i, spans[1][i])
    blocks = (first_block, second_block, third, fourth)
    for kind, s, i in plan(cols):
        blk, span = blocks[s], spans[KINDS[s]][i]
        if kind == "last":
            use(*events[5], last=True)
        elif kind == "far":
            pl.when(inner)(lambda: d_arrive(blk, i, span, (0, 1)))
        elif kind == "near":
            pl.when(inner)(lambda: d_arrive(blk, i, span, (2,)))
        elif kind == "end":
            pl.when(outer)(lambda: d_arrive(blk, i, span))
        elif kind == "use":
            if s < 2:
                pl.when(blk != z)(lambda: d_swaps(blk, i, span, 1 - y, lambda copy: copy.wait_recv()))
            else:
                d_swaps(blk, i, span, 1 - y, lambda copy: copy.wait_recv())
            make_part(blk, i, span)
        else:
            stages[direct(s, i)][kind - 1](blk, i, span)

    token_move(t, pair, 0, True).wait_send()
    for i, one in enumerate(others):
        token_move(t, one, 1 + i, False).wait_send()
    sent = lambda copy: copy.wait_send()
    own_pieces(inward, sent)

    @pl.when(inner)
    def _():
        own_pieces(outward, sent)
        own_d_pieces(0, inward, sent)
        own_d_pieces(0, outward, sent)

    pl.when(jnp.logical_not(inner))(lambda: own_d_pieces(1, inward, sent))

    for s, blk in enumerate(blocks):
        def settle():
            way = way_of(blk)
            for r in range(3):
                @pl.when(jnp.logical_and(arrives(r, way), passes(r, way)))
                def _():
                    for u in (0, 1):
                        for piece in pieces(r):
                            along(u, blk, r, piece, way).wait_send()
                    for i, span in enumerate(spans[KINDS[s]]):
                        d_along(blk, i, span, r, way).wait_send()

            for u in (0, 1):
                swaps(u, blk, y, sent)
            for i, span in enumerate(spans[KINDS[s]]):
                d_swaps(blk, i, span, y, sent)

        pl.when(blk != z)(settle)
        for i, span in enumerate(spans[KINDS[s]]):
            to_mate(blk, i, span).wait_send()
            if direct(s, i):
                line_all(blk, i, span).wait_send()
                cross_all(blk, i, span).wait_send()
            else:
                cross_one(blk, i, span).wait_send()
                line_one(blk, i, span).wait_send()
                share(blk, i, span, row).wait_send()
            give(blk, i, span, c).wait_send()
            write(blk, i, span).wait()


def fused(n, tokens, norm_gain, gate_weight, up_weight, down_weight):
    rows, width = tokens.shape
    depth, units = gate_weight.shape
    cols = down_weight.shape[1]
    held = (units + MID) // 2
    dma = pltpu.SemaphoreType.DMA
    grid_of = (n, MOST_CUTS)
    quarter = rows // 4
    hbm = pl.BlockSpec(memory_space=pl.ANY)
    vmem = pl.BlockSpec(memory_space=pltpu.VMEM)
    return pl.pallas_call(
        functools.partial(kernel, n),
        out_shape=jax.ShapeDtypeStruct((rows, width), BF16),
        in_specs=[hbm, vmem, hbm, hbm, hbm],
        out_specs=hbm,
        scratch_shapes=[
            pltpu.VMEM((rows, width), BF16),
            pltpu.VMEM((rows, width), BF16),
            pltpu.VMEM((2 * rows, width), BF16),
            pltpu.VMEM((2, n, depth, units), BF16),
            pltpu.VMEM((n, units, cols), BF16),
            pltpu.VMEM((2, 2 * rows, held), F32),
            pltpu.VMEM((2 * rows, held), BF16),
            pltpu.VMEM((n, 2, 2, 2, quarter, cols), BF16),
            pltpu.VMEM((n, 2, 2, quarter, cols), BF16),
            pltpu.VMEM((n, 2, 2, quarter, cols), BF16),
            pltpu.VMEM((n, 2, quarter, cols), BF16),
            pltpu.VMEM((n, 2, quarter, cols), BF16),
            pltpu.VMEM((n, 2, quarter, cols), BF16),
            pltpu.VMEM((rows, width), BF16),
            dma((4,)),
            dma((2, n, 3, SUBS, 2)),
            dma((2, n, 3, SUBS)),
            dma((n, MOST_CUTS, 3, 2)),
            dma((n, MOST_CUTS, 3)),
            dma((2, n, 2, SUBS)),
            dma((2, n, 2, SUBS)),
            dma((n, MOST_CUTS, 2)),
            dma((n, MOST_CUTS, 2)),
            dma((4,)),
            dma((4,)),
        ] + [dma(grid_of) for _ in range(11)],
        compiler_params=pltpu.CompilerParams(
            collective_id=0, has_side_effects=True, vmem_limit_bytes=60 * 2**20
        ),
    )(tokens, norm_gain.reshape(1, width), gate_weight, up_weight, down_weight)


def solution(mesh):
    n = mesh.shape["fs"]
    small = mesh.shape["rep"] == 2 and mesh.shape["tp"] == 4 and n == 4
    body = functools.partial(fused, n) if small else plain
    in_specs = (P(("rep", "fs"), None), P(), P("fs", "tp"), P("fs", "tp"), P("tp", "fs"))
    out_specs = P(("rep", "fs"), None)
    return jax.shard_map(
        body, mesh=mesh, in_specs=in_specs, out_specs=out_specs, check_vma=False
    )
```

```python
import functools

import jax
import jax.numpy as jnp
from jax import lax
from jax.experimental import pallas as pl
from jax.experimental.pallas import tpu as pltpu
from jax.sharding import PartitionSpec as P

MESH = pl.DeviceIdType.MESH
F32 = jnp.float32
BF16 = jnp.bfloat16


def plain(tokens, norm_gain, gate_weight, up_weight, down_weight):
    wide_tok = tokens.astype(F32)
    scale = lax.rsqrt(jnp.mean(wide_tok * wide_tok, axis=-1, keepdims=True) + 1e-06)
    normed = (wide_tok * scale * norm_gain).astype(BF16)
    gate = jnp.dot(normed, lax.all_gather(gate_weight, "fs", axis=0, tiled=True), preferred_element_type=F32)
    up = jnp.dot(normed, lax.all_gather(up_weight, "fs", axis=0, tiled=True), preferred_element_type=F32)
    hidden = (jax.nn.silu(gate) * up).astype(BF16)
    down = lax.all_gather(down_weight, "fs", axis=1, tiled=True)
    partial_value = jnp.dot(hidden, down, preferred_element_type=F32)
    return lax.psum(partial_value.astype(BF16), "tp")


CUTS = ((2, 2), (2, 1, 1))
KINDS = (1, 0, 0, 1)
DIRECT = (0, 1, 0, 1)
MOST_CUTS = 3
SUBS = 2
SLACK = 0.0
MID = 128


def spans_of(which, width):
    spans, at = [], 0
    for part in CUTS[which]:
        spans.append((at, part * width // 4))
        at += part * width // 4
    return spans


def plan(width):
    block, hop, start = 15.4, 2.2, 67.2
    free = {"x": 0.0, "z": 0.0, "weights": 71.7, "core": 74.0}
    todo = [(72.0, "last", 0, 0)]

    def book(link, when, size):
        free[link] = max(free[link], when) + size
        return free[link]

    for s in range(4):
        for i, (at, size) in enumerate(spans_of(KINDS[s], width)):
            share = block * size / width
            ready = 70.0
            if s == 1:
                out = 64.0 + block * (at + size) / width / 2 + hop
                todo.append((out, "end", s, i))
                ready = out + share / 2 + hop
            if s >= 2:
                begin = start + (s - 2) * block + block * at / width
                far, near = begin + 0.55 * share + hop, begin + share + hop
                out = book("weights", far, share / 2) + hop
                todo += [(far, "far", s, i), (near, "near", s, i), (out, "end", s, i)]
                ready = max(near, out) + share / 2 + hop
            done = book("core", ready, 1.2 * size / 256 + 0.2)
            todo.append((done, "use", s, i))
    uses = [(when, s, i) for when, kind, s, i in todo if kind == "use"]
    pend = [(when + 1.8, 1, s, i) for when, s, i in uses]
    while pend:
        pend.sort()
        when, stage, s, i = pend.pop(0)
        todo.append((when, stage, s, i))
        size = spans_of(KINDS[s], width)[i][1]
        half = block * size / width * 5.5 / 15.4
        path = ROUTES[direct(s)]
        if stage <= len(path):
            link, scale = path[stage - 1]
            after = when + 1.5 if link == "core" else book(link, when, half * scale) + hop + SLACK
            pend.append((after, stage + 1, s, i))
    todo.sort(key=lambda item: item[0])
    return [item[1:] for item in todo]


ROUTES = (
    (("x", 1.0), ("z", 0.8), ("x", 0.5), ("core", 0.0)),
    (("z", 1.0), ("x", 1.0), ("core", 0.0)),
)


def direct(s):
    return DIRECT[s]


def kernel(
    n, tok_ref, gain_ref, wg_ref, wu_ref, wd_ref, out_ref,
    tokv, tokp, normed, bw, bd, acc, hidden, part, r1, sbuf, rz, sx, r2, outv,
    loc_sem, zsend, zrecv, dsend, drecv, ysend, yrecv, vsend, vrecv, tsend, trecv,
    psend, precv, wsend, wrecv, xsend, xrecv, asend, arecv, qsend, qrecv, osem,
):
    z = lax.axis_index("fs")
    y = lax.axis_index("rep")
    t = lax.axis_index("tp")
    c = lax.rem(t, 2)
    tokens, width = tok_ref.shape
    depth, units = wg_ref.shape
    cols = wd_ref.shape[1]
    spans = tuple(spans_of(which, cols) for which in (0, 1))
    half_k, half_t, quarter = depth // 2, tokens // 2, tokens // 4
    sub_k = half_k // SUBS
    most = (units - MID) // 2
    e = lax.rem(z, 2)
    hi = z // 2
    inner = e != hi
    near = z + 1 - 2 * e
    third = 2 - hi
    fourth = 3 - 3 * hi
    pair = {"fs": near}
    has_mid = inner
    mine = pl.multiple_of(e * (most + MID), MID)
    first_unit = pl.multiple_of(e * jnp.where(has_mid, most, most + MID), MID)
    mate = {"tp": t + 1 - 2 * c}
    across = {"tp": lax.rem(t + 2, 4)}
    row = t // 2
    first_block, second_block = 3 * hi, 1 + hi
    peer = {"rep": 1 - y}

    barrier = pltpu.get_barrier_semaphore()

    around = ({"fs": lax.rem(z + 1, n)}, {"fs": lax.rem(z + n - 1, n)})
    others = tuple({"tp": lax.rem(t + d, 4)} for d in (1, 2, 3))
    for one in around + others + (peer,):
        pl.semaphore_signal(barrier, 1, device_id=one, device_id_type=MESH)
    tok_copy = pltpu.make_async_copy(tok_ref, tokv, loc_sem.at[3])
    tok_copy.start()
    pl.semaphore_wait(barrier, 6)

    def token_move(quart, to, sem, first):
        at = pl.ds(pl.multiple_of(quart * quarter, quarter), quarter)
        return pltpu.make_async_remote_copy(
            src_ref=(tok_ref if first else tokp).at[at],
            dst_ref=tokp.at[at],
            send_sem=tsend.at[sem],
            recv_sem=trecv.at[quart],
            device_id=to,
            device_id_type=MESH,
        )

    def start_of(r, way):
        if r == 1:
            return most, MID
        side = way if r == 0 else 1 - way
        return pl.multiple_of(side * (most + MID), MID), most

    def side_of(r, way):
        return way if r == 0 else 1 - way

    def kept(r, way):
        return inner if r == 1 else side_of(r, way) == e

    def passes(r, way):
        q = side_of(r, way)
        return jnp.logical_or(
            jnp.logical_and(way == 0, z > q), jnp.logical_and(way == 1, z < n - 2 + q))

    def arrives(r, way):
        q = side_of(r, way)
        return jnp.logical_or(
            jnp.logical_and(way == 0, z >= q), jnp.logical_and(way == 1, z < n - 1 + q))

    def pieces(r):
        return range(1 if r == 1 else SUBS)

    def rows_of(r, s, who):
        if r == 1:
            return pl.ds(pl.multiple_of(who * half_k, half_k), half_k)
        return pl.ds(pl.multiple_of(who * half_k + s * sub_k, sub_k), sub_k)

    def along(u, blk, r, s, way, own=None):
        start, size = start_of(r, way)
        at = (rows_of(r, s, y), pl.ds(start, size))
        return pltpu.make_async_remote_copy(
            src_ref=bw.at[(u, blk) + at] if own is None else own.at[at],
            dst_ref=bw.at[(u, blk) + at],
            send_sem=zsend.at[blk, way],
            recv_sem=zrecv.at[u, blk, (0, SUBS, SUBS + 1)[r] + s],
            device_id={"fs": z - 1 + 2 * way},
            device_id_type=MESH,
        )

    def swap(u, blk, i, s, who):
        start, size = ((mine, most), (most, MID))[i]
        place = bw.at[u, blk, rows_of(i, s, who), pl.ds(start, size)]
        return pltpu.make_async_remote_copy(
            src_ref=place,
            dst_ref=place,
            send_sem=ysend.at[blk],
            recv_sem=yrecv.at[u, blk],
            device_id=peer,
            device_id_type=MESH,
        )

    def d_rows(start, size, who):
        return pl.ds(pl.multiple_of(start + who * (size // 2), 64), size // 2)

    def d_along(blk, i, span, r, way, own=False):
        start, size = start_of(r, way)
        at = (d_rows(start, size, y), pl.ds(*span))
        return pltpu.make_async_remote_copy(
            src_ref=wd_ref.at[at] if own else bd.at[(blk,) + at],
            dst_ref=bd.at[(blk,) + at],
            send_sem=dsend.at[blk, way],
            recv_sem=drecv.at[blk, i, r],
            device_id={"fs": z - 1 + 2 * way},
            device_id_type=MESH,
        )

    def d_swap(blk, i, span, p, who):
        start, size = ((mine, most), (most, MID))[p]
        place = bd.at[blk, d_rows(start, size, who), pl.ds(*span)]
        return pltpu.make_async_remote_copy(
            src_ref=place,
            dst_ref=place,
            send_sem=vsend.at[blk],
            recv_sem=vrecv.at[blk, i],
            device_id=peer,
            device_id_type=MESH,
        )

    def own_pieces(way, body):
        for u, own in ((0, wg_ref), (1, wu_ref)):
            for r in range(3):
                @pl.when(passes(r, way))
                def _():
                    for s in pieces(r):
                        body(along(u, z, r, s, way, own))

    def own_d_pieces(which, way, body):
        for i, span in enumerate(spans[which]):
            for r in range(3):
                pl.when(passes(r, way))(lambda: body(d_along(z, i, span, r, way, True)))

    go = lambda copy: copy.start()
    ZERO, ONE = jnp.int32(0), jnp.int32(1)
    inward, outward = 1 - hi, hi
    @pl.when(inner)
    def _():
        own_pieces(inward, go)
        token_move(t, pair, 0, True).start()
        own_pieces(outward, go)

    @pl.when(jnp.logical_not(inner))
    def _():
        token_move(t, pair, 0, True).start()
        own_pieces(inward, go)
        own_d_pieces(1, inward, go)

    locals_ = [
        pltpu.make_async_copy(wg_ref, bw.at[0, z], loc_sem.at[0]),
        pltpu.make_async_copy(wu_ref, bw.at[1, z], loc_sem.at[1]),
        pltpu.make_async_copy(wd_ref, bd.at[z], loc_sem.at[2]),
    ]
    for copy in locals_:
        copy.start()

    step = 64

    def norm(src, base):
        @pl.loop(0, tokens // step)
        def _(i):
            at = pl.ds(pl.multiple_of(i * step, step), step)
            to = pl.ds(pl.multiple_of(base + i * step, step), step)
            wide = src[at, :].astype(F32)
            scale = lax.rsqrt(jnp.mean(wide * wide, axis=-1, keepdims=True) + 1e-06)
            normed[to, :] = (wide * scale * gain_ref[...]).astype(BF16)

    def by_size(body):
        pl.when(has_mid)(lambda: body(most + MID))
        pl.when(jnp.logical_not(has_mid))(lambda: body(most))

    def add_dot(u, blk, first=False, last=False, start=0, rows=None):
        rows = depth if rows is None else rows

        def piece(size):
            to = pl.ds(0, size)

            @pl.loop(0, 4)
            def _(i):
                at = pl.ds(pl.multiple_of(i * half_t, half_t), half_t)
                left = normed[at, pl.ds(pl.multiple_of(blk * depth + start, rows), rows)]
                right = bw[u, blk, pl.ds(pl.multiple_of(start, rows), rows), pl.ds(first_unit, size)]
                value = jnp.dot(left, right, preferred_element_type=F32)
                if first:
                    acc[u, at, to] = value
                elif last:
                    hidden[at, to] = (acc[0, at, to] * (acc[1, at, to] + value)).astype(BF16)
                else:
                    acc[u, at, to] = acc[u, at, to] + value

        by_size(piece)

    def activate():
        def piece(size):
            to = pl.ds(0, size)

            @pl.loop(0, 2 * tokens // step)
            def _(i):
                at = pl.ds(pl.multiple_of(i * step, step), step)
                value = acc[0, at, to]
                acc[0, at, to] = value / (1.0 + jnp.exp(-value))

        by_size(piece)

    def place(blk, span, start, size):
        return (
            pl.ds(pl.multiple_of(start, size), size),
            pl.ds(pl.multiple_of(blk * cols + span[0], 128), span[1]),
        )

    def remote(src, dst, sems, at, to):
        return pltpu.make_async_remote_copy(
            src, dst, sems[0].at[at[0]], sems[1].at[at], device_id=to, device_id_type=MESH)

    def to_mate(blk, i, span):
        return remote(part.at[blk, 1, :, :, :, pl.ds(*span)], r1.at[blk, :, :, :, pl.ds(*span)], (psend, precv), (blk, i), mate)

    def line_all(blk, i, span):
        return remote(sbuf.at[blk, 1, :, :, pl.ds(*span)], rz.at[blk, :, :, pl.ds(*span)], (wsend, wrecv), (blk, i), pair)

    def line_one(blk, i, span):
        return remote(sx.at[blk, 1, :, pl.ds(*span)], rz.at[blk, 0, :, pl.ds(*span)], (wsend, wrecv), (blk, i), pair)

    def cross_all(blk, i, span):
        return remote(sx.at[blk, :, :, pl.ds(*span)], r2.at[blk, :, :, pl.ds(*span)], (xsend, xrecv), (blk, i), across)

    def cross_one(blk, i, span):
        return remote(sbuf.at[blk, :, 1 - row, :, pl.ds(*span)], r2.at[blk, :, :, pl.ds(*span)], (xsend, xrecv), (blk, i), across)

    def share(blk, i, span, who):
        at = outv.at[place(blk, span, c * half_t + who * quarter, quarter)]
        return remote(at, at, (asend, arecv), (blk, i), across)

    def give(blk, i, span, who):
        at = outv.at[place(blk, span, who * half_t, half_t)]
        return remote(at, at, (qsend, qrecv), (blk, i), mate)

    def write(blk, i, span):
        at = pl.ds(pl.multiple_of(blk * cols + span[0], 128), span[1])
        return pltpu.make_async_copy(outv.at[:, at], out_ref.at[:, at], osem.at[blk])

    def make_part(blk, i, span):
        def fill(size, side):
            @pl.loop(0, 2)
            def _(which):
                whose = c + side - 2 * c * side
                at = pl.ds(pl.multiple_of(which * tokens + whose * half_t, half_t), half_t)
                value = jnp.dot(
                    hidden[at, pl.ds(0, size)], bd[blk, pl.ds(first_unit, size), pl.ds(*span)],
                    preferred_element_type=F32)
                part[blk, side, which, :, :, pl.ds(*span)] = value.astype(BF16).reshape(2, quarter, span[1])

        by_size(lambda size: fill(size, 1))
        to_mate(blk, i, span).start()
        by_size(lambda size: fill(size, 0))

    def sum_mate(blk, i, span):
        to_mate(blk, i, span).wait_recv()
        at = pl.ds(*span)
        sbuf[blk, :, :, :, at] = (part[blk, 0, :, :, :, at].astype(F32) + r1[blk, :, :, :, at].astype(F32)).astype(BF16)

    def direct_1(blk, i, span):
        sum_mate(blk, i, span)
        line_all(blk, i, span).start()

    def direct_2(blk, i, span):
        line_all(blk, i, span).wait_recv()
        at = pl.ds(*span)
        sx[blk, :, :, at] = (sbuf[blk, 0, :, :, at].astype(F32) + rz[blk, :, :, at].astype(F32)).astype(BF16)
        cross_all(blk, i, span).start()

    def direct_3(blk, i, span):
        cross_all(blk, i, span).wait_recv()
        at = pl.ds(*span)
        value = (sx[blk, :, :, at].astype(F32) + r2[blk, :, :, at].astype(F32)).astype(BF16)
        outv[place(blk, span, c * half_t, half_t)] = value.reshape(half_t, span[1])
        give(blk, i, span, c).start()

    def split_1(blk, i, span):
        sum_mate(blk, i, span)
        cross_one(blk, i, span).start()

    def split_2(blk, i, span):
        cross_one(blk, i, span).wait_recv()
        at = pl.ds(*span)
        sx[blk, :, :, at] = (sbuf[blk, :, row, :, at].astype(F32) + r2[blk, :, :, at].astype(F32)).astype(BF16)
        line_one(blk, i, span).start()

    def split_3(blk, i, span):
        line_one(blk, i, span).wait_recv()
        at = pl.ds(*span)
        outv[place(blk, span, c * half_t + row * quarter, quarter)] = (
            sx[blk, 0, :, at].astype(F32) + rz[blk, 0, :, at].astype(F32)).astype(BF16)
        share(blk, i, span, row).start()

    def split_4(blk, i, span):
        share(blk, i, span, 1 - row).wait_recv()
        give(blk, i, span, c).start()

    def store(blk, i, span):
        give(blk, i, span, 1 - c).wait_recv()
        write(blk, i, span).start()

    stages = ((split_1, split_2, split_3, split_4, store), (direct_1, direct_2, direct_3, store))

    def way_of(blk):
        return jnp.where(blk < z, ONE, ZERO)

    def arrive(u, blk, rs=(0, 1, 2)):
        way = way_of(blk)
        for r in rs:
            @pl.when(arrives(r, way))
            def _():
                for s in pieces(r):
                    along(u, blk, r, s, way).wait_recv()
                    pl.when(passes(r, way))(lambda: along(u, blk, r, s, way).start())
                    pl.when(kept(r, way))(lambda: swap(u, blk, int(r == 1), s, y).start())

    def all_received(ref, sem):
        pltpu.make_async_remote_copy(ref, ref, zsend.at[0, 0], sem, device_id=peer, device_id_type=MESH).wait_recv()

    def all_sent(ref, sem):
        pltpu.make_async_remote_copy(ref, ref, sem, zrecv.at[0, 0, 0], device_id=peer, device_id_type=MESH).wait_send()

    def swapped(u, blk):
        rows = pl.ds(pl.multiple_of((1 - y) * half_k, half_k), half_k)
        by_size(lambda size: all_received(bw.at[u, blk, rows, pl.ds(first_unit, size)], yrecv.at[u, blk]))

    def d_arrive(blk, i, span, rs=(0, 1, 2)):
        way = way_of(blk)
        for r in rs:
            @pl.when(arrives(r, way))
            def _():
                d_along(blk, i, span, r, way).wait_recv()
                pl.when(passes(r, way))(lambda: d_along(blk, i, span, r, way).start())
                pl.when(kept(r, way))(lambda: d_swap(blk, i, span, int(r == 1), y).start())

    def d_swapped(blk, i, span):
        by_size(lambda size: all_received(bd.at[blk, pl.ds(0, size // 2), pl.ds(*span)], vrecv.at[blk, i]))

    def use(u, blk, last=False):
        if last:
            add_dot(u, blk, start=y * half_k, rows=half_k)
            swapped(u, blk)
            add_dot(u, blk, last=True, start=(1 - y) * half_k, rows=half_k)
        else:
            swapped(u, blk)
            add_dot(u, blk)

    zero_in = jnp.where(inner, ZERO, ONE)
    events = (
        (ZERO, jnp.where(inner, third, near)),
        (zero_in, near),
        (1 - zero_in, third),
        (ONE, jnp.where(inner, near, third)),
        (ZERO, fourth),
        (ONE, fourth),
    )

    tok_copy.wait()
    norm(tokv, 0)
    for copy in locals_:
        copy.wait()
    token_move(t, pair, 0, True).wait_recv()
    for i, one in enumerate(others):
        token_move(t, one, 1 + i, False).start()
    outer = jnp.logical_not(inner)
    arrive(*events[0])
    arrive(*events[1])
    arrive(*events[2])
    for d in (1, 2, 3):
        token_move(lax.rem(t + d, 4), mate, 0, False).wait_recv()
    norm(tokp, tokens)
    pl.when(inner)(lambda: arrive(*events[3], rs=(0,)))
    for u in (0, 1):
        add_dot(u, z, first=True)
    pl.when(inner)(lambda: arrive(*events[4], rs=(0, 1)))
    pl.when(outer)(lambda: arrive(*events[3]))
    use(*events[0])

    @pl.when(inner)
    def _():
        arrive(*events[3], rs=(1, 2))
        own_d_pieces(0, inward, go)

    use(*events[1])
    use(*events[2])
    pl.when(inner)(lambda: arrive(*events[4], rs=(2,)))
    pl.when(outer)(lambda: arrive(*events[4]))
    use(*events[3])

    @pl.when(inner)
    def _():
        d_arrive(first_block, 0, spans[1][0])
        arrive(*events[5], rs=(0,))

    use(*events[4])

    @pl.when(inner)
    def _():
        arrive(*events[5], rs=(1,))
        own_d_pieces(0, outward, go)

    activate()
    pl.when(outer)(lambda: arrive(*events[5]))

    @pl.when(inner)
    def _():
        arrive(*events[5], rs=(2,))
        for i in range(1, len(spans[1])):
            d_arrive(first_block, i, spans[1][i])
    blocks = (first_block, second_block, third, fourth)
    for kind, s, i in plan(cols):
        blk, span = blocks[s], spans[KINDS[s]][i]
        if kind == "last":
            use(*events[5], last=True)
        elif kind == "far":
            pl.when(inner)(lambda: d_arrive(blk, i, span, (0, 1)))
        elif kind == "near":
            pl.when(inner)(lambda: d_arrive(blk, i, span, (2,)))
        elif kind == "end":
            pl.when(outer)(lambda: d_arrive(blk, i, span))
        elif kind == "use":
            if s < 2:
                pl.when(blk != z)(lambda: d_swapped(blk, i, span))
            else:
                d_swapped(blk, i, span)
            make_part(blk, i, span)
        else:
            stages[direct(s)][kind - 1](blk, i, span)

    token_move(t, pair, 0, True).wait_send()
    for i, one in enumerate(others):
        token_move(t, one, 1 + i, False).wait_send()

    def sent_along(blk, way):
        def wait(size):
            all_sent(bw.at[:, blk, pl.ds(0, half_k), pl.ds(0, size)], zsend.at[blk, way])
            all_sent(bd.at[blk, pl.ds(0, size // 2)], dsend.at[blk, way])

        some = jnp.logical_and(passes(0, way), jnp.logical_not(passes(2, way)))
        pl.when(passes(2, way))(lambda: wait(units))
        pl.when(jnp.logical_and(some, passes(1, way)))(lambda: wait(most + MID))
        pl.when(jnp.logical_and(some, jnp.logical_not(passes(1, way))))(lambda: wait(most))

    def sent_swap(blk):
        def wait(size):
            all_sent(bw.at[:, blk, pl.ds(0, half_k), pl.ds(0, size)], ysend.at[blk])
            all_sent(bd.at[blk, pl.ds(0, size // 2)], vsend.at[blk])

        by_size(wait)

    sent_along(z, ZERO)
    sent_along(z, ONE)
    whole = (0, cols)
    for s, blk in enumerate(blocks):
        def settle():
            sent_along(blk, way_of(blk))
            sent_swap(blk)

        pl.when(blk != z)(settle)
        all_sent(part.at[blk, 1], psend.at[blk])
        if direct(s):
            all_sent(sbuf.at[blk, 1], wsend.at[blk])
            all_sent(sx.at[blk], xsend.at[blk])
        else:
            all_sent(sbuf.at[blk, :, 0], xsend.at[blk])
            all_sent(sx.at[blk, 1], wsend.at[blk])
            all_sent(outv.at[place(blk, whole, 0, quarter)], asend.at[blk])
        all_sent(outv.at[place(blk, whole, 0, half_t)], qsend.at[blk])
        write(blk, 0, whole).wait()


def fused(n, tokens, norm_gain, gate_weight, up_weight, down_weight):
    rows, width = tokens.shape
    depth, units = gate_weight.shape
    cols = down_weight.shape[1]
    held = (units + MID) // 2
    dma = pltpu.SemaphoreType.DMA
    quarter = rows // 4
    hbm = pl.BlockSpec(memory_space=pl.ANY)
    vmem = pl.BlockSpec(memory_space=pltpu.VMEM)
    return pl.pallas_call(
        functools.partial(kernel, n),
        out_shape=jax.ShapeDtypeStruct((rows, width), BF16),
        in_specs=[hbm, vmem, hbm, hbm, hbm],
        out_specs=hbm,
        scratch_shapes=[
            pltpu.VMEM((rows, width), BF16),
            pltpu.VMEM((rows, width), BF16),
            pltpu.VMEM((2 * rows, width), BF16),
            pltpu.VMEM((2, n, depth, units), BF16),
            pltpu.VMEM((n, units, cols), BF16),
            pltpu.VMEM((2, 2 * rows, held), F32),
            pltpu.VMEM((2 * rows, held), BF16),
            pltpu.VMEM((n, 2, 2, 2, quarter, cols), BF16),
            pltpu.VMEM((n, 2, 2, quarter, cols), BF16),
            pltpu.VMEM((n, 2, 2, quarter, cols), BF16),
            pltpu.VMEM((n, 2, quarter, cols), BF16),
            pltpu.VMEM((n, 2, quarter, cols), BF16),
            pltpu.VMEM((n, 2, quarter, cols), BF16),
            pltpu.VMEM((rows, width), BF16),
            dma((4,)),
            dma((n, 2)),
            dma((2, n, 2 * SUBS + 1)),
            dma((n, 2)),
            dma((n, MOST_CUTS, 3)),
            dma((n,)),
            dma((2, n)),
            dma((n,)),
            dma((n, MOST_CUTS)),
            dma((4,)),
            dma((4,)),
        ] + 5 * [dma((n,)), dma((n, MOST_CUTS))] + [dma((n,))],
        compiler_params=pltpu.CompilerParams(
            collective_id=0, has_side_effects=True, vmem_limit_bytes=60 * 2**20
        ),
    )(tokens, norm_gain.reshape(1, width), gate_weight, up_weight, down_weight)


def solution(mesh):
    n = mesh.shape["fs"]
    small = mesh.shape["rep"] == 2 and mesh.shape["tp"] == 4 and n == 4
    body = functools.partial(fused, n) if small else plain
    in_specs = (P(("rep", "fs"), None), P(), P("fs", "tp"), P("fs", "tp"), P("tp", "fs"))
    out_specs = P(("rep", "fs"), None)
    return jax.shard_map(
        body, mesh=mesh, in_specs=in_specs, out_specs=out_specs, check_vma=False
    )
```

```python
import functools

import jax
import jax.numpy as jnp
from jax import lax
from jax.experimental import pallas as pl
from jax.experimental.pallas import tpu as pltpu
from jax.sharding import PartitionSpec as P

MESH = pl.DeviceIdType.MESH
F32 = jnp.float32
BF16 = jnp.bfloat16


def plain(tokens, norm_gain, gate_weight, up_weight, down_weight):
    wide_tok = tokens.astype(F32)
    scale = lax.rsqrt(jnp.mean(wide_tok * wide_tok, axis=-1, keepdims=True) + 1e-06)
    normed = (wide_tok * scale * norm_gain).astype(BF16)
    gate = jnp.dot(normed, lax.all_gather(gate_weight, "fs", axis=0, tiled=True), preferred_element_type=F32)
    up = jnp.dot(normed, lax.all_gather(up_weight, "fs", axis=0, tiled=True), preferred_element_type=F32)
    hidden = (jax.nn.silu(gate) * up).astype(BF16)
    down = lax.all_gather(down_weight, "fs", axis=1, tiled=True)
    partial_value = jnp.dot(hidden, down, preferred_element_type=F32)
    return lax.psum(partial_value.astype(BF16), "tp")


CUTS = (1, 1, 1, 1)
DIRECT = (0, 0, 0, 1)
MOST_CUTS = 4
SUBS = 2
MID = 128


def spans_of(width):
    spans, at = [], 0
    for part in CUTS:
        spans.append((at, part * width // 4))
        at += part * width // 4
    return spans


ORDER = (
    ("end", 1, 0), ("last", 0, 0), ("far", 2, 0), ("far", 2, 1), ("near", 2, 0), ("end", 1, 1), ("use", 0, 1),
    ("use", 0, 3), (1, 0, 1), ("use", 1, 0), (1, 1, 0), (1, 0, 3), ("end", 1, 2), ("far", 2, 2),
    ("use", 1, 1), ("near", 2, 1), ("end", 1, 3), ("end", 2, 0), ("use", 0, 0), ("near", 2, 2), ("use", 0, 2),
    (2, 1, 0), (1, 0, 0), ("far", 2, 3), (1, 0, 2), (2, 0, 1), ("end", 2, 1), ("use", 1, 3), ("use", 1, 2),
    ("far", 3, 0), ("near", 2, 3), (2, 0, 3), (1, 1, 1), ("use", 2, 0), ("end", 2, 2), (2, 0, 0),
    ("near", 3, 0), (1, 1, 3), ("use", 2, 1), (1, 2, 0), ("far", 3, 1), (2, 0, 2), (1, 1, 2), ("end", 2, 3),
    (2, 1, 1), ("end", 3, 0), (3, 0, 0), ("use", 2, 2), ("near", 3, 1), (2, 1, 3), ("far", 3, 2), (1, 2, 1),
    (2, 1, 2), (2, 2, 0), ("end", 3, 1), (1, 2, 2), ("use", 2, 3), (3, 0, 1), ("use", 3, 0), (1, 2, 3),
    ("end", 3, 2), (4, 0, 0), ("far", 3, 3), ("near", 3, 2), (3, 1, 0), (1, 3, 0), ("use", 3, 1), (3, 0, 2),
    (3, 0, 3), ("near", 3, 3), (3, 1, 2), (3, 1, 1), (1, 3, 1), (2, 2, 1), ("end", 3, 3), (3, 2, 0),
    (5, 0, 0), (2, 2, 2), ("use", 3, 2), (2, 2, 3), (4, 0, 2), (4, 0, 1), (2, 3, 0), (2, 3, 1), (1, 3, 2),
    (4, 1, 0), (3, 1, 3), (3, 2, 1), ("use", 3, 3), (4, 0, 3), (3, 2, 2), (1, 3, 3), (5, 0, 3), (3, 2, 3),
    (5, 0, 1), (4, 1, 1), (2, 3, 2), (4, 2, 0), (2, 3, 3), (3, 3, 1), (3, 3, 0), (4, 1, 2), (4, 3, 0),
    (4, 2, 3), (4, 1, 3), (4, 2, 2), (5, 1, 2), (3, 3, 2), (4, 3, 1), (5, 0, 2), (5, 2, 2), (5, 1, 0),
    (5, 2, 3), (5, 2, 0), (5, 1, 1), (4, 2, 1), (3, 3, 3), (4, 3, 2), (5, 1, 3), (5, 2, 1), (4, 3, 3),
)


def direct(s):
    return DIRECT[s]


def kernel(
    n, tok_ref, gain_ref, wg_ref, wu_ref, wd_ref, out_ref,
    tokv, tokp, normed, bw, bd, acc, hidden, part, r1, sbuf, rz, sx, r2, outv,
    loc_sem, zsend, zrecv, dsend, drecv, ysend, yrecv, vsend, vrecv, tsend, trecv,
    psend, precv, wsend, wrecv, xsend, xrecv, asend, arecv, qsend, qrecv, osem,
):
    z = lax.axis_index("fs")
    y = lax.axis_index("rep")
    t = lax.axis_index("tp")
    c = lax.rem(t, 2)
    tokens, width = tok_ref.shape
    depth, units = wg_ref.shape
    cols = wd_ref.shape[1]
    spans = spans_of(cols)
    half_k, half_t, quarter = depth // 2, tokens // 2, tokens // 4
    sub_k = half_k // SUBS
    most = (units - MID) // 2
    e = lax.rem(z, 2)
    hi = z // 2
    inner = e != hi
    near = z + 1 - 2 * e
    third = 2 - hi
    fourth = 3 - 3 * hi
    pair = {"fs": near}
    has_mid = inner
    mine = pl.multiple_of(e * (most + MID), MID)
    first_unit = pl.multiple_of(e * jnp.where(has_mid, most, most + MID), MID)
    mate = {"tp": t + 1 - 2 * c}
    across = {"tp": lax.rem(t + 2, 4)}
    row = t // 2
    peer = {"rep": 1 - y}

    barrier = pltpu.get_barrier_semaphore()

    around = ({"fs": lax.rem(z + 1, n)}, {"fs": lax.rem(z + n - 1, n)})
    others = tuple({"tp": lax.rem(t + d, 4)} for d in (1, 2, 3))
    for one in around + others + (peer,):
        pl.semaphore_signal(barrier, 1, device_id=one, device_id_type=MESH)
    tok_copy = pltpu.make_async_copy(tok_ref, tokv, loc_sem.at[3])
    tok_copy.start()
    pl.semaphore_wait(barrier, 6)

    def token_move(quart, to, sem, first):
        at = pl.ds(pl.multiple_of(quart * quarter, quarter), quarter)
        return pltpu.make_async_remote_copy(
            src_ref=(tok_ref if first else tokp).at[at],
            dst_ref=tokp.at[at],
            send_sem=tsend.at[sem],
            recv_sem=trecv.at[quart],
            device_id=to,
            device_id_type=MESH,
        )

    def start_of(r, way):
        if r == 1:
            return most, MID
        side = way if r == 0 else 1 - way
        return pl.multiple_of(side * (most + MID), MID), most

    def side_of(r, way):
        return way if r == 0 else 1 - way

    def kept(r, way):
        return inner if r == 1 else side_of(r, way) == e

    def passes(r, way):
        q = side_of(r, way)
        return jnp.logical_or(
            jnp.logical_and(way == 0, z > q), jnp.logical_and(way == 1, z < n - 2 + q))

    def arrives(r, way):
        q = side_of(r, way)
        return jnp.logical_or(
            jnp.logical_and(way == 0, z >= q), jnp.logical_and(way == 1, z < n - 1 + q))

    def pieces(r):
        return range(1 if r == 1 else SUBS)

    def rows_of(r, s, who):
        if r == 1:
            return pl.ds(pl.multiple_of(who * half_k, half_k), half_k)
        return pl.ds(pl.multiple_of(who * half_k + s * sub_k, sub_k), sub_k)

    def along(u, blk, r, s, way, own=None):
        start, size = start_of(r, way)
        at = (rows_of(r, s, y), pl.ds(start, size))
        return pltpu.make_async_remote_copy(
            src_ref=bw.at[(u, blk) + at] if own is None else own.at[at],
            dst_ref=bw.at[(u, blk) + at],
            send_sem=zsend.at[blk, way],
            recv_sem=zrecv.at[u, blk, (0, SUBS, SUBS + 1)[r] + s],
            device_id={"fs": z - 1 + 2 * way},
            device_id_type=MESH,
        )

    def swap(u, blk, i, s, who):
        start, size = ((mine, most), (most, MID))[i]
        place = bw.at[u, blk, rows_of(i, s, who), pl.ds(start, size)]
        return pltpu.make_async_remote_copy(
            src_ref=place,
            dst_ref=place,
            send_sem=ysend.at[blk],
            recv_sem=yrecv.at[u, blk],
            device_id=peer,
            device_id_type=MESH,
        )

    def d_rows(start, size, who):
        return pl.ds(pl.multiple_of(start + who * (size // 2), 64), size // 2)

    def d_along(blk, i, span, r, way, own=False):
        start, size = start_of(r, way)
        at = (d_rows(start, size, y), pl.ds(*span))
        return pltpu.make_async_remote_copy(
            src_ref=wd_ref.at[at] if own else bd.at[(blk,) + at],
            dst_ref=bd.at[(blk,) + at],
            send_sem=dsend.at[blk, way],
            recv_sem=drecv.at[blk, i, r],
            device_id={"fs": z - 1 + 2 * way},
            device_id_type=MESH,
        )

    def d_swap(blk, i, span, p, who):
        start, size = ((mine, most), (most, MID))[p]
        place = bd.at[blk, d_rows(start, size, who), pl.ds(*span)]
        return pltpu.make_async_remote_copy(
            src_ref=place,
            dst_ref=place,
            send_sem=vsend.at[blk],
            recv_sem=vrecv.at[blk, i],
            device_id=peer,
            device_id_type=MESH,
        )

    def own_pieces(way, body):
        for u, own in ((0, wg_ref), (1, wu_ref)):
            for r in range(3):
                @pl.when(passes(r, way))
                def _():
                    for s in pieces(r):
                        body(along(u, z, r, s, way, own))

    def own_d_pieces(way, body):
        for i, span in enumerate(spans):
            for r in range(3):
                pl.when(passes(r, way))(lambda: body(d_along(z, i, span, r, way, True)))

    go = lambda copy: copy.start()
    ZERO, ONE = jnp.int32(0), jnp.int32(1)
    inward, outward = 1 - hi, hi
    @pl.when(inner)
    def _():
        own_pieces(inward, go)
        token_move(t, pair, 0, True).start()
        own_pieces(outward, go)

    @pl.when(jnp.logical_not(inner))
    def _():
        token_move(t, pair, 0, True).start()
        own_pieces(inward, go)
        own_d_pieces(inward, go)

    locals_ = [
        pltpu.make_async_copy(wg_ref, bw.at[0, z], loc_sem.at[0]),
        pltpu.make_async_copy(wu_ref, bw.at[1, z], loc_sem.at[1]),
        pltpu.make_async_copy(wd_ref, bd.at[z], loc_sem.at[2]),
    ]
    for copy in locals_:
        copy.start()

    step = 64

    def norm(src, base):
        @pl.loop(0, tokens // step)
        def _(i):
            at = pl.ds(pl.multiple_of(i * step, step), step)
            to = pl.ds(pl.multiple_of(base + i * step, step), step)
            wide = src[at, :].astype(F32)
            scale = lax.rsqrt(jnp.mean(wide * wide, axis=-1, keepdims=True) + 1e-06)
            normed[to, :] = (wide * scale * gain_ref[...]).astype(BF16)

    def by_size(body):
        pl.when(has_mid)(lambda: body(most + MID))
        pl.when(jnp.logical_not(has_mid))(lambda: body(most))

    def add_dot(u, blk, first=False, last=False, start=0, rows=None):
        rows = depth if rows is None else rows

        def piece(size):
            to = pl.ds(0, size)

            @pl.loop(0, 4)
            def _(i):
                at = pl.ds(pl.multiple_of(i * half_t, half_t), half_t)
                left = normed[at, pl.ds(pl.multiple_of(blk * depth + start, rows), rows)]
                right = bw[u, blk, pl.ds(pl.multiple_of(start, rows), rows), pl.ds(first_unit, size)]
                value = jnp.dot(left, right, preferred_element_type=F32)
                if first:
                    acc[u, at, to] = value
                elif last:
                    hidden[at, to] = (acc[0, at, to] * (acc[1, at, to] + value)).astype(BF16)
                else:
                    acc[u, at, to] = acc[u, at, to] + value

        by_size(piece)

    def activate():
        def piece(size):
            to = pl.ds(0, size)

            @pl.loop(0, 2 * tokens // step)
            def _(i):
                at = pl.ds(pl.multiple_of(i * step, step), step)
                value = acc[0, at, to]
                acc[0, at, to] = value / (1.0 + jnp.exp(-value))

        by_size(piece)

    def place(blk, span, start, size):
        return (
            pl.ds(pl.multiple_of(start, size), size),
            pl.ds(pl.multiple_of(blk * cols + span[0], 128), span[1]),
        )

    def remote(src, dst, sems, at, to):
        return pltpu.make_async_remote_copy(
            src, dst, sems[0].at[at[0]], sems[1].at[at], device_id=to, device_id_type=MESH)

    def to_mate(blk, i, span):
        return remote(part.at[blk, 1, :, :, :, pl.ds(*span)], r1.at[blk, :, :, :, pl.ds(*span)], (psend, precv), (blk, i), mate)

    def line_all(blk, i, span):
        return remote(sbuf.at[blk, 1, :, :, pl.ds(*span)], rz.at[blk, :, :, pl.ds(*span)], (wsend, wrecv), (blk, i), pair)

    def line_one(blk, i, span):
        return remote(sx.at[blk, 1, :, pl.ds(*span)], rz.at[blk, 0, :, pl.ds(*span)], (wsend, wrecv), (blk, i), pair)

    def cross_all(blk, i, span):
        return remote(sx.at[blk, :, :, pl.ds(*span)], r2.at[blk, :, :, pl.ds(*span)], (xsend, xrecv), (blk, i), across)

    def cross_one(blk, i, span):
        return remote(sbuf.at[blk, :, 1 - row, :, pl.ds(*span)], r2.at[blk, :, :, pl.ds(*span)], (xsend, xrecv), (blk, i), across)

    def share(blk, i, span, who):
        at = outv.at[place(blk, span, c * half_t + who * quarter, quarter)]
        return remote(at, at, (asend, arecv), (blk, i), across)

    def give(blk, i, span, who):
        at = outv.at[place(blk, span, who * half_t, half_t)]
        return remote(at, at, (qsend, qrecv), (blk, i), mate)

    def write(blk, i, span):
        at = pl.ds(pl.multiple_of(blk * cols + span[0], 128), span[1])
        return pltpu.make_async_copy(outv.at[:, at], out_ref.at[:, at], osem.at[blk])

    def make_part(blk, i, span):
        def fill(size, side):
            @pl.loop(0, 2)
            def _(which):
                whose = c + side - 2 * c * side
                at = pl.ds(pl.multiple_of(which * tokens + whose * half_t, half_t), half_t)
                value = jnp.dot(
                    hidden[at, pl.ds(0, size)], bd[blk, pl.ds(first_unit, size), pl.ds(*span)],
                    preferred_element_type=F32)
                part[blk, side, which, :, :, pl.ds(*span)] = value.astype(BF16).reshape(2, quarter, span[1])

        by_size(lambda size: fill(size, 1))
        to_mate(blk, i, span).start()
        by_size(lambda size: fill(size, 0))

    def sum_mate(blk, i, span):
        to_mate(blk, i, span).wait_recv()
        at = pl.ds(*span)
        sbuf[blk, :, :, :, at] = (part[blk, 0, :, :, :, at].astype(F32) + r1[blk, :, :, :, at].astype(F32)).astype(BF16)

    def direct_1(blk, i, span):
        sum_mate(blk, i, span)
        line_all(blk, i, span).start()

    def direct_2(blk, i, span):
        line_all(blk, i, span).wait_recv()
        at = pl.ds(*span)
        sx[blk, :, :, at] = (sbuf[blk, 0, :, :, at].astype(F32) + rz[blk, :, :, at].astype(F32)).astype(BF16)
        cross_all(blk, i, span).start()

    def direct_3(blk, i, span):
        cross_all(blk, i, span).wait_recv()
        at = pl.ds(*span)
        value = (sx[blk, :, :, at].astype(F32) + r2[blk, :, :, at].astype(F32)).astype(BF16)
        outv[place(blk, span, c * half_t, half_t)] = value.reshape(half_t, span[1])
        give(blk, i, span, c).start()

    def split_1(blk, i, span):
        sum_mate(blk, i, span)
        cross_one(blk, i, span).start()

    def split_2(blk, i, span):
        cross_one(blk, i, span).wait_recv()
        at = pl.ds(*span)
        sx[blk, :, :, at] = (sbuf[blk, :, row, :, at].astype(F32) + r2[blk, :, :, at].astype(F32)).astype(BF16)
        line_one(blk, i, span).start()

    def split_3(blk, i, span):
        line_one(blk, i, span).wait_recv()
        at = pl.ds(*span)
        outv[place(blk, span, c * half_t + row * quarter, quarter)] = (
            sx[blk, 0, :, at].astype(F32) + rz[blk, 0, :, at].astype(F32)).astype(BF16)
        share(blk, i, span, row).start()

    def split_4(blk, i, span):
        share(blk, i, span, 1 - row).wait_recv()
        give(blk, i, span, c).start()

    def store(blk, i, span):
        give(blk, i, span, 1 - c).wait_recv()
        write(blk, i, span).start()

    stages = ((split_1, split_2, split_3, split_4, store), (direct_1, direct_2, direct_3, store))

    def way_of(blk):
        return jnp.where(blk < z, ONE, ZERO)

    def arrive(u, blk, rs=(0, 1, 2)):
        way = way_of(blk)
        for r in rs:
            @pl.when(arrives(r, way))
            def _():
                for s in pieces(r):
                    along(u, blk, r, s, way).wait_recv()
                    pl.when(passes(r, way))(lambda: along(u, blk, r, s, way).start())
                    pl.when(kept(r, way))(lambda: swap(u, blk, int(r == 1), s, y).start())

    def all_received(ref, sem):
        pltpu.make_async_remote_copy(ref, ref, zsend.at[0, 0], sem, device_id=peer, device_id_type=MESH).wait_recv()

    def all_sent(ref, sem):
        pltpu.make_async_remote_copy(ref, ref, sem, zrecv.at[0, 0, 0], device_id=peer, device_id_type=MESH).wait_send()

    def swapped(u, blk):
        rows = pl.ds(pl.multiple_of((1 - y) * half_k, half_k), half_k)
        by_size(lambda size: all_received(bw.at[u, blk, rows, pl.ds(first_unit, size)], yrecv.at[u, blk]))

    def d_arrive(blk, i, span, rs=(0, 1, 2)):
        way = way_of(blk)
        for r in rs:
            @pl.when(arrives(r, way))
            def _():
                d_along(blk, i, span, r, way).wait_recv()
                pl.when(passes(r, way))(lambda: d_along(blk, i, span, r, way).start())
                pl.when(kept(r, way))(lambda: d_swap(blk, i, span, int(r == 1), y).start())

    def d_swapped(blk, i, span):
        by_size(lambda size: all_received(bd.at[blk, pl.ds(0, size // 2), pl.ds(*span)], vrecv.at[blk, i]))

    def use(u, blk, last=False):
        if last:
            add_dot(u, blk, start=y * half_k, rows=half_k)
            swapped(u, blk)
            add_dot(u, blk, last=True, start=(1 - y) * half_k, rows=half_k)
        else:
            swapped(u, blk)
            add_dot(u, blk)

    zero_in = jnp.where(inner, ZERO, ONE)
    events = (
        (ZERO, jnp.where(inner, third, near)),
        (zero_in, near),
        (1 - zero_in, third),
        (ONE, jnp.where(inner, near, third)),
        (ZERO, fourth),
        (ONE, fourth),
    )

    tok_copy.wait()
    norm(tokv, 0)
    for copy in locals_:
        copy.wait()
    token_move(t, pair, 0, True).wait_recv()
    for i, one in enumerate(others):
        token_move(t, one, 1 + i, False).start()
    outer = jnp.logical_not(inner)
    arrive(*events[0])
    arrive(*events[1])
    arrive(*events[2])
    for d in (1, 2, 3):
        token_move(lax.rem(t + d, 4), mate, 0, False).wait_recv()
    norm(tokp, tokens)
    pl.when(inner)(lambda: arrive(*events[3], rs=(0,)))
    for u in (0, 1):
        add_dot(u, z, first=True)
    pl.when(inner)(lambda: arrive(*events[4], rs=(0, 1)))
    pl.when(outer)(lambda: arrive(*events[3]))
    use(*events[0])

    @pl.when(inner)
    def _():
        arrive(*events[3], rs=(1, 2))
        own_d_pieces(inward, go)

    use(*events[1])
    use(*events[2])
    pl.when(inner)(lambda: arrive(*events[4], rs=(2,)))
    pl.when(outer)(lambda: arrive(*events[4]))
    use(*events[3])

    @pl.when(inner)
    def _():
        arrive(*events[5], rs=(0,))

    use(*events[4])

    @pl.when(inner)
    def _():
        arrive(*events[5], rs=(1,))
        own_d_pieces(outward, go)

    activate()
    pl.when(outer)(lambda: arrive(*events[5]))

    @pl.when(inner)
    def _():
        arrive(*events[5], rs=(2,))
        for i, span in enumerate(spans):
            d_arrive(near, i, span)
    blocks = (z, near, third, fourth)
    for kind, s, i in ORDER:
        blk, span = blocks[s], spans[i]
        if kind == "last":
            use(*events[5], last=True)
        elif kind == "far":
            pl.when(inner)(lambda: d_arrive(blk, i, span, (0, 1)))
        elif kind == "near":
            pl.when(inner)(lambda: d_arrive(blk, i, span, (2,)))
        elif kind == "end":
            pl.when(outer)(lambda: d_arrive(blk, i, span))
        elif kind == "use":
            if s > 0:
                d_swapped(blk, i, span)
            make_part(blk, i, span)
        else:
            stages[direct(s)][kind - 1](blk, i, span)

    token_move(t, pair, 0, True).wait_send()
    for i, one in enumerate(others):
        token_move(t, one, 1 + i, False).wait_send()

    def sent_along(blk, way):
        def wait(size):
            all_sent(bw.at[:, blk, pl.ds(0, half_k), pl.ds(0, size)], zsend.at[blk, way])
            all_sent(bd.at[blk, pl.ds(0, size // 2)], dsend.at[blk, way])

        some = jnp.logical_and(passes(0, way), jnp.logical_not(passes(2, way)))
        pl.when(passes(2, way))(lambda: wait(units))
        pl.when(jnp.logical_and(some, passes(1, way)))(lambda: wait(most + MID))
        pl.when(jnp.logical_and(some, jnp.logical_not(passes(1, way))))(lambda: wait(most))

    def sent_swap(blk):
        def wait(size):
            all_sent(bw.at[:, blk, pl.ds(0, half_k), pl.ds(0, size)], ysend.at[blk])
            all_sent(bd.at[blk, pl.ds(0, size // 2)], vsend.at[blk])

        by_size(wait)

    sent_along(z, ZERO)
    sent_along(z, ONE)
    whole = (0, cols)
    for s, blk in enumerate(blocks):
        def settle():
            sent_along(blk, way_of(blk))
            sent_swap(blk)

        if s > 0:
            settle()
        all_sent(part.at[blk, 1], psend.at[blk])
        if direct(s):
            all_sent(sbuf.at[blk, 1], wsend.at[blk])
            all_sent(sx.at[blk], xsend.at[blk])
        else:
            all_sent(sbuf.at[blk, :, 0], xsend.at[blk])
            all_sent(sx.at[blk, 1], wsend.at[blk])
            all_sent(outv.at[place(blk, whole, 0, quarter)], asend.at[blk])
        all_sent(outv.at[place(blk, whole, 0, half_t)], qsend.at[blk])
        write(blk, 0, whole).wait()


def fused(n, tokens, norm_gain, gate_weight, up_weight, down_weight):
    rows, width = tokens.shape
    depth, units = gate_weight.shape
    cols = down_weight.shape[1]
    held = (units + MID) // 2
    dma = pltpu.SemaphoreType.DMA
    quarter = rows // 4
    hbm = pl.BlockSpec(memory_space=pl.ANY)
    vmem = pl.BlockSpec(memory_space=pltpu.VMEM)
    return pl.pallas_call(
        functools.partial(kernel, n),
        out_shape=jax.ShapeDtypeStruct((rows, width), BF16),
        in_specs=[hbm, vmem, hbm, hbm, hbm],
        out_specs=hbm,
        scratch_shapes=[
            pltpu.VMEM((rows, width), BF16),
            pltpu.VMEM((rows, width), BF16),
            pltpu.VMEM((2 * rows, width), BF16),
            pltpu.VMEM((2, n, depth, units), BF16),
            pltpu.VMEM((n, units, cols), BF16),
            pltpu.VMEM((2, 2 * rows, held), F32),
            pltpu.VMEM((2 * rows, held), BF16),
            pltpu.VMEM((n, 2, 2, 2, quarter, cols), BF16),
            pltpu.VMEM((n, 2, 2, quarter, cols), BF16),
            pltpu.VMEM((n, 2, 2, quarter, cols), BF16),
            pltpu.VMEM((n, 2, quarter, cols), BF16),
            pltpu.VMEM((n, 2, quarter, cols), BF16),
            pltpu.VMEM((n, 2, quarter, cols), BF16),
            pltpu.VMEM((rows, width), BF16),
            dma((4,)),
            dma((n, 2)),
            dma((2, n, 2 * SUBS + 1)),
            dma((n, 2)),
            dma((n, MOST_CUTS, 3)),
            dma((n,)),
            dma((2, n)),
            dma((n,)),
            dma((n, MOST_CUTS)),
            dma((4,)),
            dma((4,)),
        ] + 5 * [dma((n,)), dma((n, MOST_CUTS))] + [dma((n,))],
        compiler_params=pltpu.CompilerParams(
            collective_id=0, has_side_effects=True, vmem_limit_bytes=60 * 2**20
        ),
    )(tokens, norm_gain.reshape(1, width), gate_weight, up_weight, down_weight)


def solution(mesh):
    n = mesh.shape["fs"]
    small = mesh.shape["rep"] == 2 and mesh.shape["tp"] == 4 and n == 4
    body = functools.partial(fused, n) if small else plain
    in_specs = (P(("rep", "fs"), None), P(), P("fs", "tp"), P("fs", "tp"), P("tp", "fs"))
    out_specs = P(("rep", "fs"), None)
    return jax.shard_map(
        body, mesh=mesh, in_specs=in_specs, out_specs=out_specs, check_vma=False
    )
```

```python
import functools

import jax
import jax.numpy as jnp
from jax import lax
from jax.experimental import pallas as pl
from jax.experimental.pallas import tpu as pltpu
from jax.sharding import PartitionSpec as P

MESH = pl.DeviceIdType.MESH
F32 = jnp.float32
BF16 = jnp.bfloat16


def plain(tokens, norm_gain, gate_weight, up_weight, down_weight):
    wide_tok = tokens.astype(F32)
    scale = lax.rsqrt(jnp.mean(wide_tok * wide_tok, axis=-1, keepdims=True) + 1e-06)
    normed = (wide_tok * scale * norm_gain).astype(BF16)
    gate = jnp.dot(normed, lax.all_gather(gate_weight, "fs", axis=0, tiled=True), preferred_element_type=F32)
    up = jnp.dot(normed, lax.all_gather(up_weight, "fs", axis=0, tiled=True), preferred_element_type=F32)
    hidden = (jax.nn.silu(gate) * up).astype(BF16)
    down = lax.all_gather(down_weight, "fs", axis=1, tiled=True)
    partial_value = jnp.dot(hidden, down, preferred_element_type=F32)
    return lax.psum(partial_value.astype(BF16), "tp")


CUTS = (1, 1, 1, 1)
DIRECT = (0, 0, 0, 1)
MOST_CUTS = 4
SUBS = 2
MID = 128


def spans_of(width):
    spans, at = [], 0
    for part in CUTS:
        spans.append((at, part * width // 4))
        at += part * width // 4
    return spans


ORDER = (
    ("end", 1, 0), ("last", 0, 0), ("far", 2, 0), ("far", 2, 1), ("near", 2, 0), ("end", 1, 1), ("use", 0, 1),
    ("use", 0, 3), (1, 0, 1), ("use", 1, 0), (1, 1, 0), (1, 0, 3), ("end", 1, 2), ("far", 2, 2),
    ("use", 1, 1), ("near", 2, 1), ("end", 1, 3), ("end", 2, 0), ("use", 0, 0), ("near", 2, 2), ("use", 0, 2),
    (2, 1, 0), (1, 0, 0), ("far", 2, 3), (1, 0, 2), (2, 0, 1), ("end", 2, 1), ("use", 1, 3), ("use", 1, 2),
    ("far", 3, 0), ("near", 2, 3), (2, 0, 3), (1, 1, 1), ("use", 2, 0), ("end", 2, 2), (2, 0, 0),
    ("near", 3, 0), (1, 1, 3), ("use", 2, 1), (1, 2, 0), ("far", 3, 1), (2, 0, 2), (1, 1, 2), ("end", 2, 3),
    (2, 1, 1), ("end", 3, 0), (3, 0, 0), ("use", 2, 2), ("near", 3, 1), (2, 1, 3), ("far", 3, 2), (1, 2, 1),
    (2, 1, 2), (2, 2, 0), ("end", 3, 1), (1, 2, 2), ("use", 2, 3), (3, 0, 1), ("use", 3, 0), (1, 2, 3),
    ("end", 3, 2), (4, 0, 0), ("far", 3, 3), ("near", 3, 2), (3, 1, 0), (1, 3, 0), ("use", 3, 1), (3, 0, 2),
    (3, 0, 3), ("near", 3, 3), (3, 1, 2), (3, 1, 1), (1, 3, 1), (2, 2, 1), ("end", 3, 3), (3, 2, 0),
    (5, 0, 0), (2, 2, 2), ("use", 3, 2), (2, 2, 3), (4, 0, 2), (4, 0, 1), (2, 3, 0), (2, 3, 1), (1, 3, 2),
    (4, 1, 0), (3, 1, 3), (3, 2, 1), ("use", 3, 3), (4, 0, 3), (3, 2, 2), (1, 3, 3), (5, 0, 3), (3, 2, 3),
    (5, 0, 1), (4, 1, 1), (2, 3, 2), (4, 2, 0), (2, 3, 3), (3, 3, 1), (3, 3, 0), (4, 1, 2), (4, 3, 0),
    (4, 2, 3), (4, 1, 3), (4, 2, 2), (5, 1, 2), (3, 3, 2), (4, 3, 1), (5, 0, 2), (5, 2, 2), (5, 1, 0),
    (5, 2, 3), (5, 2, 0), (5, 1, 1), (4, 2, 1), (3, 3, 3), (4, 3, 2), (5, 1, 3), (5, 2, 1), (4, 3, 3),
)


def direct(s):
    return DIRECT[s]


def kernel(
    n, tok_ref, gain_ref, wg_ref, wu_ref, wd_ref, out_ref,
    tokv, tokp, normed, bw, bd, acc, hidden, part, r1, sbuf, rz, sx, r2, outv,
    loc_sem, zsend, zrecv, dsend, drecv, ysend, yrecv, vsend, vrecv, tsend, trecv,
    psend, precv, wsend, wrecv, xsend, xrecv, asend, arecv, qsend, qrecv, osem,
):
    z = lax.axis_index("fs")
    y = lax.axis_index("rep")
    t = lax.axis_index("tp")
    c = lax.rem(t, 2)
    tokens, width = tok_ref.shape
    depth, units = wg_ref.shape
    cols = wd_ref.shape[1]
    spans = spans_of(cols)
    half_k, half_t, quarter = depth // 2, tokens // 2, tokens // 4
    sub_k = half_k // SUBS
    most = (units - MID) // 2
    e = lax.rem(z, 2)
    hi = z // 2
    inner = e != hi
    near = z + 1 - 2 * e
    third = 2 - hi
    fourth = 3 - 3 * hi
    pair = {"fs": near}
    has_mid = inner
    mine = pl.multiple_of(e * (most + MID), MID)
    first_unit = pl.multiple_of(e * jnp.where(has_mid, most, most + MID), MID)
    mate = {"tp": t + 1 - 2 * c}
    across = {"tp": lax.rem(t + 2, 4)}
    row = t // 2
    peer = {"rep": 1 - y}

    barrier = pltpu.get_barrier_semaphore()

    around = ({"fs": lax.rem(z + 1, n)}, {"fs": lax.rem(z + n - 1, n)})
    others = tuple({"tp": lax.rem(t + d, 4)} for d in (1, 2, 3))
    for one in around + others + (peer,):
        pl.semaphore_signal(barrier, 1, device_id=one, device_id_type=MESH)
    tok_copy = pltpu.make_async_copy(tok_ref, tokv, loc_sem.at[3])
    tok_copy.start()
    pl.semaphore_wait(barrier, 6)

    def token_move(quart, to, sem, first):
        at = pl.ds(pl.multiple_of(quart * quarter, quarter), quarter)
        return pltpu.make_async_remote_copy(
            src_ref=(tok_ref if first else tokp).at[at],
            dst_ref=tokp.at[at],
            send_sem=tsend.at[sem],
            recv_sem=trecv.at[quart],
            device_id=to,
            device_id_type=MESH,
        )

    def start_of(r, way):
        if r == 1:
            return most, MID
        side = way if r == 0 else 1 - way
        return pl.multiple_of(side * (most + MID), MID), most

    def side_of(r, way):
        return way if r == 0 else 1 - way

    def kept(r, way):
        return inner if r == 1 else side_of(r, way) == e

    def passes(r, way):
        q = side_of(r, way)
        return jnp.logical_or(
            jnp.logical_and(way == 0, z > q), jnp.logical_and(way == 1, z < n - 2 + q))

    def arrives(r, way):
        q = side_of(r, way)
        return jnp.logical_or(
            jnp.logical_and(way == 0, z >= q), jnp.logical_and(way == 1, z < n - 1 + q))

    def pieces(r):
        return range(1 if r == 1 else SUBS)

    def rows_of(r, s, who):
        if r == 1:
            return pl.ds(pl.multiple_of(who * half_k, half_k), half_k)
        return pl.ds(pl.multiple_of(who * half_k + s * sub_k, sub_k), sub_k)

    def along(u, blk, r, s, way, own=None):
        start, size = start_of(r, way)
        at = (rows_of(r, s, y), pl.ds(start, size))
        return pltpu.make_async_remote_copy(
            src_ref=bw.at[(u, blk) + at] if own is None else own.at[at],
            dst_ref=bw.at[(u, blk) + at],
            send_sem=zsend.at[blk, way],
            recv_sem=zrecv.at[u, blk, (0, SUBS, SUBS + 1)[r] + s],
            device_id={"fs": z - 1 + 2 * way},
            device_id_type=MESH,
        )

    def swap(u, blk, i, s, who):
        start, size = ((mine, most), (most, MID))[i]
        place = bw.at[u, blk, rows_of(i, s, who), pl.ds(start, size)]
        return pltpu.make_async_remote_copy(
            src_ref=place,
            dst_ref=place,
            send_sem=ysend.at[blk],
            recv_sem=yrecv.at[u, blk],
            device_id=peer,
            device_id_type=MESH,
        )

    def d_rows(start, size, who):
        return pl.ds(pl.multiple_of(start + who * (size // 2), 64), size // 2)

    def d_along(blk, i, span, r, way, own=False):
        start, size = start_of(r, way)
        at = (d_rows(start, size, y), pl.ds(*span))
        return pltpu.make_async_remote_copy(
            src_ref=wd_ref.at[at] if own else bd.at[(blk,) + at],
            dst_ref=bd.at[(blk,) + at],
            send_sem=dsend.at[blk, way],
            recv_sem=drecv.at[blk, i, r],
            device_id={"fs": z - 1 + 2 * way},
            device_id_type=MESH,
        )

    def d_swap(blk, i, span, p, who):
        start, size = ((mine, most), (most, MID))[p]
        place = bd.at[blk, d_rows(start, size, who), pl.ds(*span)]
        return pltpu.make_async_remote_copy(
            src_ref=place,
            dst_ref=place,
            send_sem=vsend.at[blk],
            recv_sem=vrecv.at[blk, i],
            device_id=peer,
            device_id_type=MESH,
        )

    def own_pieces(way, body):
        for u, own in ((0, wg_ref), (1, wu_ref)):
            for r in range(3):
                @pl.when(passes(r, way))
                def _():
                    for s in pieces(r):
                        body(along(u, z, r, s, way, own))

    def own_d_pieces(way, body):
        for i, span in enumerate(spans):
            for r in range(3):
                pl.when(passes(r, way))(lambda: body(d_along(z, i, span, r, way, True)))

    go = lambda copy: copy.start()
    ZERO, ONE = jnp.int32(0), jnp.int32(1)
    inward, outward = 1 - hi, hi
    @pl.when(inner)
    def _():
        own_pieces(inward, go)
        token_move(t, pair, 0, True).start()
        own_pieces(outward, go)

    @pl.when(jnp.logical_not(inner))
    def _():
        token_move(t, pair, 0, True).start()
        own_pieces(inward, go)
        own_d_pieces(inward, go)

    locals_ = [
        pltpu.make_async_copy(wg_ref, bw.at[0, z], loc_sem.at[0]),
        pltpu.make_async_copy(wu_ref, bw.at[1, z], loc_sem.at[1]),
        pltpu.make_async_copy(wd_ref, bd.at[z], loc_sem.at[2]),
    ]
    for copy in locals_:
        copy.start()

    step = 64

    def norm(src, base):
        @pl.loop(0, tokens // step)
        def _(i):
            at = pl.ds(pl.multiple_of(i * step, step), step)
            to = pl.ds(pl.multiple_of(base + i * step, step), step)
            wide = src[at, :].astype(F32)
            scale = lax.rsqrt(jnp.mean(wide * wide, axis=-1, keepdims=True) + 1e-06)
            normed[to, :] = (wide * scale * gain_ref[...]).astype(BF16)

    def by_size(body):
        pl.when(has_mid)(lambda: body(most + MID))
        pl.when(jnp.logical_not(has_mid))(lambda: body(most))

    def add_dot(u, blk, first=False, last=False, start=0, rows=None):
        rows = depth if rows is None else rows

        def piece(size):
            to = pl.ds(0, size)

            @pl.loop(0, 4)
            def _(i):
                at = pl.ds(pl.multiple_of(i * half_t, half_t), half_t)
                left = normed[at, pl.ds(pl.multiple_of(blk * depth + start, rows), rows)]
                right = bw[u, blk, pl.ds(pl.multiple_of(start, rows), rows), pl.ds(first_unit, size)]
                value = jnp.dot(left, right, preferred_element_type=F32)
                if first:
                    acc[u, at, to] = value
                elif last:
                    hidden[at, to] = (acc[0, at, to] * (acc[1, at, to] + value)).astype(BF16)
                else:
                    acc[u, at, to] = acc[u, at, to] + value

        by_size(piece)

    def activate():
        def piece(size):
            to = pl.ds(0, size)

            @pl.loop(0, 2 * tokens // step)
            def _(i):
                at = pl.ds(pl.multiple_of(i * step, step), step)
                value = acc[0, at, to]
                acc[0, at, to] = value / (1.0 + jnp.exp(-value))

        by_size(piece)

    def place(blk, span, start, size):
        return (
            pl.ds(pl.multiple_of(start, size), size),
            pl.ds(pl.multiple_of(blk * cols + span[0], 128), span[1]),
        )

    def remote(src, dst, sems, at, to):
        return pltpu.make_async_remote_copy(
            src, dst, sems[0].at[at[0]], sems[1].at[at], device_id=to, device_id_type=MESH)

    def to_mate(blk, i, span):
        return remote(part.at[blk, 1, :, :, :, pl.ds(*span)], r1.at[blk, :, :, :, pl.ds(*span)], (psend, precv), (blk, i), mate)

    def line_all(blk, i, span):
        return remote(sbuf.at[blk, 1, :, :, pl.ds(*span)], rz.at[blk, :, :, pl.ds(*span)], (wsend, wrecv), (blk, i), pair)

    def line_one(blk, i, span):
        return remote(sx.at[blk, 1, :, pl.ds(*span)], rz.at[blk, 0, :, pl.ds(*span)], (wsend, wrecv), (blk, i), pair)

    def cross_all(blk, i, span):
        return remote(sx.at[blk, :, :, pl.ds(*span)], r2.at[blk, :, :, pl.ds(*span)], (xsend, xrecv), (blk, i), across)

    def cross_one(blk, i, span):
        return remote(sbuf.at[blk, :, 1 - row, :, pl.ds(*span)], r2.at[blk, :, :, pl.ds(*span)], (xsend, xrecv), (blk, i), across)

    def share(blk, i, span, who):
        at = outv.at[place(blk, span, c * half_t + who * quarter, quarter)]
        return remote(at, at, (asend, arecv), (blk, i), across)

    def give(blk, i, span, who):
        at = outv.at[place(blk, span, who * half_t, half_t)]
        return remote(at, at, (qsend, qrecv), (blk, i), mate)

    def write(blk, i, span):
        at = pl.ds(pl.multiple_of(blk * cols + span[0], 128), span[1])
        return pltpu.make_async_copy(outv.at[:, at], out_ref.at[:, at], osem.at[blk])

    def make_part(blk, i, span):
        def fill(size, side):
            @pl.loop(0, 2)
            def _(which):
                whose = c + side - 2 * c * side
                at = pl.ds(pl.multiple_of(which * tokens + whose * half_t, half_t), half_t)
                value = jnp.dot(
                    hidden[at, pl.ds(0, size)], bd[blk, pl.ds(first_unit, size), pl.ds(*span)],
                    preferred_element_type=F32)
                part[blk, side, which, :, :, pl.ds(*span)] = value.astype(BF16).reshape(2, quarter, span[1])

        by_size(lambda size: fill(size, 1))
        to_mate(blk, i, span).start()
        by_size(lambda size: fill(size, 0))

    def sum_mate(blk, i, span):
        to_mate(blk, i, span).wait_recv()
        at = pl.ds(*span)
        sbuf[blk, :, :, :, at] = (part[blk, 0, :, :, :, at].astype(F32) + r1[blk, :, :, :, at].astype(F32)).astype(BF16)

    def direct_1(blk, i, span):
        sum_mate(blk, i, span)
        line_all(blk, i, span).start()

    def direct_2(blk, i, span):
        line_all(blk, i, span).wait_recv()
        at = pl.ds(*span)
        sx[blk, :, :, at] = (sbuf[blk, 0, :, :, at].astype(F32) + rz[blk, :, :, at].astype(F32)).astype(BF16)
        cross_all(blk, i, span).start()

    def direct_3(blk, i, span):
        cross_all(blk, i, span).wait_recv()
        at = pl.ds(*span)
        value = (sx[blk, :, :, at].astype(F32) + r2[blk, :, :, at].astype(F32)).astype(BF16)
        outv[place(blk, span, c * half_t, half_t)] = value.reshape(half_t, span[1])
        give(blk, i, span, c).start()

    def split_1(blk, i, span):
        sum_mate(blk, i, span)
        cross_one(blk, i, span).start()

    def split_2(blk, i, span):
        cross_one(blk, i, span).wait_recv()
        at = pl.ds(*span)
        sx[blk, :, :, at] = (sbuf[blk, :, row, :, at].astype(F32) + r2[blk, :, :, at].astype(F32)).astype(BF16)
        line_one(blk, i, span).start()

    def split_3(blk, i, span):
        line_one(blk, i, span).wait_recv()
        at = pl.ds(*span)
        outv[place(blk, span, c * half_t + row * quarter, quarter)] = (
            sx[blk, 0, :, at].astype(F32) + rz[blk, 0, :, at].astype(F32)).astype(BF16)
        share(blk, i, span, row).start()

    def split_4(blk, i, span):
        share(blk, i, span, 1 - row).wait_recv()
        give(blk, i, span, c).start()

    def store(blk, i, span):
        give(blk, i, span, 1 - c).wait_recv()
        write(blk, i, span).start()

    stages = ((split_1, split_2, split_3, split_4, store), (direct_1, direct_2, direct_3, store))

    def way_of(blk):
        return jnp.where(blk < z, ONE, ZERO)

    def arrive(u, blk, rs=(0, 1, 2)):
        way = way_of(blk)
        for r in rs:
            @pl.when(arrives(r, way))
            def _():
                for s in pieces(r):
                    along(u, blk, r, s, way).wait_recv()
                    pl.when(passes(r, way))(lambda: along(u, blk, r, s, way).start())
                    pl.when(kept(r, way))(lambda: swap(u, blk, int(r == 1), s, y).start())

    def all_received(ref, sem):
        pltpu.make_async_remote_copy(ref, ref, zsend.at[0, 0], sem, device_id=peer, device_id_type=MESH).wait_recv()

    def all_sent(ref, sem):
        pltpu.make_async_remote_copy(ref, ref, sem, zrecv.at[0, 0, 0], device_id=peer, device_id_type=MESH).wait_send()

    def swapped(u, blk):
        rows = pl.ds(pl.multiple_of((1 - y) * half_k, half_k), half_k)
        by_size(lambda size: all_received(bw.at[u, blk, rows, pl.ds(first_unit, size)], yrecv.at[u, blk]))

    def d_arrive(blk, i, span, rs=(0, 1, 2)):
        way = way_of(blk)
        for r in rs:
            @pl.when(arrives(r, way))
            def _():
                d_along(blk, i, span, r, way).wait_recv()
                pl.when(passes(r, way))(lambda: d_along(blk, i, span, r, way).start())
                pl.when(kept(r, way))(lambda: d_swap(blk, i, span, int(r == 1), y).start())

    def d_swapped(blk, i, span):
        by_size(lambda size: all_received(bd.at[blk, pl.ds(0, size // 2), pl.ds(*span)], vrecv.at[blk, i]))

    def use(u, blk, last=False):
        if last:
            add_dot(u, blk, start=y * half_k, rows=half_k)
            swapped(u, blk)
            add_dot(u, blk, last=True, start=(1 - y) * half_k, rows=half_k)
        else:
            swapped(u, blk)
            add_dot(u, blk)

    zero_in = jnp.where(inner, ZERO, ONE)
    events = (
        (ZERO, jnp.where(inner, third, near)),
        (zero_in, near),
        (1 - zero_in, third),
        (ONE, jnp.where(inner, near, third)),
        (ZERO, fourth),
        (ONE, fourth),
    )

    tok_copy.wait()
    norm(tokv, 0)
    for copy in locals_:
        copy.wait()
    pl.when(inner)(lambda: arrive(*events[0]))
    token_move(t, pair, 0, True).wait_recv()
    for i, one in enumerate(others):
        token_move(t, one, 1 + i, False).start()
    outer = jnp.logical_not(inner)
    pl.when(outer)(lambda: arrive(*events[0]))
    arrive(*events[1])
    arrive(*events[2])
    for d in (1, 2, 3):
        token_move(lax.rem(t + d, 4), mate, 0, False).wait_recv()
    norm(tokp, tokens)
    pl.when(inner)(lambda: arrive(*events[3], rs=(0,)))
    for u in (0, 1):
        add_dot(u, z, first=True)
    pl.when(inner)(lambda: arrive(*events[4], rs=(0, 1)))
    pl.when(outer)(lambda: arrive(*events[3]))
    use(*events[0])

    @pl.when(inner)
    def _():
        arrive(*events[3], rs=(1, 2))
        own_d_pieces(inward, go)

    use(*events[1])
    use(*events[2])
    pl.when(inner)(lambda: arrive(*events[4], rs=(2,)))
    pl.when(outer)(lambda: arrive(*events[4]))
    use(*events[3])

    @pl.when(inner)
    def _():
        arrive(*events[5], rs=(0,))

    use(*events[4])

    @pl.when(inner)
    def _():
        arrive(*events[5], rs=(1,))
        own_d_pieces(outward, go)

    activate()
    pl.when(outer)(lambda: arrive(*events[5]))

    @pl.when(inner)
    def _():
        arrive(*events[5], rs=(2,))
        for i, span in enumerate(spans):
            d_arrive(near, i, span)
    blocks = (z, near, third, fourth)
    for kind, s, i in ORDER:
        blk, span = blocks[s], spans[i]
        if kind == "last":
            use(*events[5], last=True)
        elif kind == "far":
            pl.when(inner)(lambda: d_arrive(blk, i, span, (0, 1)))
        elif kind == "near":
            pl.when(inner)(lambda: d_arrive(blk, i, span, (2,)))
        elif kind == "end":
            pl.when(outer)(lambda: d_arrive(blk, i, span))
        elif kind == "use":
            if s > 0:
                d_swapped(blk, i, span)
            make_part(blk, i, span)
        else:
            stages[direct(s)][kind - 1](blk, i, span)

    token_move(t, pair, 0, True).wait_send()
    for i, one in enumerate(others):
        token_move(t, one, 1 + i, False).wait_send()

    def sent_along(blk, way):
        def wait(size):
            all_sent(bw.at[:, blk, pl.ds(0, half_k), pl.ds(0, size)], zsend.at[blk, way])
            all_sent(bd.at[blk, pl.ds(0, size // 2)], dsend.at[blk, way])

        some = jnp.logical_and(passes(0, way), jnp.logical_not(passes(2, way)))
        pl.when(passes(2, way))(lambda: wait(units))
        pl.when(jnp.logical_and(some, passes(1, way)))(lambda: wait(most + MID))
        pl.when(jnp.logical_and(some, jnp.logical_not(passes(1, way))))(lambda: wait(most))

    def sent_swap(blk):
        def wait(size):
            all_sent(bw.at[:, blk, pl.ds(0, half_k), pl.ds(0, size)], ysend.at[blk])
            all_sent(bd.at[blk, pl.ds(0, size // 2)], vsend.at[blk])

        by_size(wait)

    sent_along(z, ZERO)
    sent_along(z, ONE)
    whole = (0, cols)
    for s, blk in enumerate(blocks):
        def settle():
            sent_along(blk, way_of(blk))
            sent_swap(blk)

        if s > 0:
            settle()
        all_sent(part.at[blk, 1], psend.at[blk])
        if direct(s):
            all_sent(sbuf.at[blk, 1], wsend.at[blk])
            all_sent(sx.at[blk], xsend.at[blk])
        else:
            all_sent(sbuf.at[blk, :, 0], xsend.at[blk])
            all_sent(sx.at[blk, 1], wsend.at[blk])
            all_sent(outv.at[place(blk, whole, 0, quarter)], asend.at[blk])
        all_sent(outv.at[place(blk, whole, 0, half_t)], qsend.at[blk])
        write(blk, 0, whole).wait()


def fused(n, tokens, norm_gain, gate_weight, up_weight, down_weight):
    rows, width = tokens.shape
    depth, units = gate_weight.shape
    cols = down_weight.shape[1]
    held = (units + MID) // 2
    dma = pltpu.SemaphoreType.DMA
    quarter = rows // 4
    hbm = pl.BlockSpec(memory_space=pl.ANY)
    vmem = pl.BlockSpec(memory_space=pltpu.VMEM)
    return pl.pallas_call(
        functools.partial(kernel, n),
        out_shape=pltpu.VMEM((rows, width), BF16),
        in_specs=[hbm, vmem, hbm, hbm, hbm],
        out_specs=hbm,
        scratch_shapes=[
            pltpu.VMEM((rows, width), BF16),
            pltpu.VMEM((rows, width), BF16),
            pltpu.VMEM((2 * rows, width), BF16),
            pltpu.VMEM((2, n, depth, units), BF16),
            pltpu.VMEM((n, units, cols), BF16),
            pltpu.VMEM((2, 2 * rows, held), F32),
            pltpu.VMEM((2 * rows, held), BF16),
            pltpu.VMEM((n, 2, 2, 2, quarter, cols), BF16),
            pltpu.VMEM((n, 2, 2, quarter, cols), BF16),
            pltpu.VMEM((n, 2, 2, quarter, cols), BF16),
            pltpu.VMEM((n, 2, quarter, cols), BF16),
            pltpu.VMEM((n, 2, quarter, cols), BF16),
            pltpu.VMEM((n, 2, quarter, cols), BF16),
            pltpu.VMEM((rows, width), BF16),
            dma((4,)),
            dma((n, 2)),
            dma((2, n, 2 * SUBS + 1)),
            dma((n, 2)),
            dma((n, MOST_CUTS, 3)),
            dma((n,)),
            dma((2, n)),
            dma((n,)),
            dma((n, MOST_CUTS)),
            dma((4,)),
            dma((4,)),
        ] + 5 * [dma((n,)), dma((n, MOST_CUTS))] + [dma((n,))],
        compiler_params=pltpu.CompilerParams(
            collective_id=0, has_side_effects=True, vmem_limit_bytes=60 * 2**20
        ),
    )(tokens, norm_gain.reshape(1, width), gate_weight, up_weight, down_weight)


def solution(mesh):
    n = mesh.shape["fs"]
    small = mesh.shape["rep"] == 2 and mesh.shape["tp"] == 4 and n == 4
    body = functools.partial(fused, n) if small else plain
    in_specs = (P(("rep", "fs"), None), P(), P("fs", "tp"), P("fs", "tp"), P("tp", "fs"))
    out_specs = P(("rep", "fs"), None)
    return jax.shard_map(
        body, mesh=mesh, in_specs=in_specs, out_specs=out_specs, check_vma=False
    )
```

```python
import functools

import jax
import jax.numpy as jnp
from jax import lax
from jax.experimental import pallas as pl
from jax.experimental.pallas import tpu as pltpu
from jax.sharding import PartitionSpec as P

MESH = pl.DeviceIdType.MESH
F32 = jnp.float32
BF16 = jnp.bfloat16


def plain(tokens, norm_gain, gate_weight, up_weight, down_weight):
    wide_tok = tokens.astype(F32)
    scale = lax.rsqrt(jnp.mean(wide_tok * wide_tok, axis=-1, keepdims=True) + 1e-06)
    normed = (wide_tok * scale * norm_gain).astype(BF16)
    gate = jnp.dot(normed, lax.all_gather(gate_weight, "fs", axis=0, tiled=True), preferred_element_type=F32)
    up = jnp.dot(normed, lax.all_gather(up_weight, "fs", axis=0, tiled=True), preferred_element_type=F32)
    hidden = (jax.nn.silu(gate) * up).astype(BF16)
    down = lax.all_gather(down_weight, "fs", axis=1, tiled=True)
    partial_value = jnp.dot(hidden, down, preferred_element_type=F32)
    return lax.psum(partial_value.astype(BF16), "tp")


CUTS = (1, 1, 1, 1)
DIRECT = (0, 0, 0, 1)
MOST_CUTS = 4
SUBS = 2
MID = 128


def spans_of(width):
    spans, at = [], 0
    for part in CUTS:
        spans.append((at, part * width // 4))
        at += part * width // 4
    return spans


ORDER = (
    ("end", 1, 0), ("last", 0, 0), ("far", 2, 0), ("far", 2, 1), ("near", 2, 0), ("end", 1, 1), ("use", 0, 1),
    ("use", 0, 3), (1, 0, 1), ("use", 1, 0), (1, 1, 0), (1, 0, 3), ("end", 1, 2), ("far", 2, 2),
    ("use", 1, 1), ("near", 2, 1), ("end", 1, 3), ("end", 2, 0), ("use", 0, 0), ("near", 2, 2), ("use", 0, 2),
    (2, 1, 0), (1, 0, 0), ("far", 2, 3), (1, 0, 2), (2, 0, 1), ("end", 2, 1), ("use", 1, 3), ("use", 1, 2),
    ("far", 3, 0), ("near", 2, 3), (2, 0, 3), (1, 1, 1), ("use", 2, 0), ("end", 2, 2), (2, 0, 0),
    ("near", 3, 0), (1, 1, 3), ("use", 2, 1), (1, 2, 0), ("far", 3, 1), (2, 0, 2), (1, 1, 2), ("end", 2, 3),
    (2, 1, 1), ("end", 3, 0), (3, 0, 0), ("use", 2, 2), ("near", 3, 1), (2, 1, 3), ("far", 3, 2), (1, 2, 1),
    (2, 1, 2), (2, 2, 0), ("end", 3, 1), (1, 2, 2), ("use", 2, 3), (3, 0, 1), ("use", 3, 0), (1, 2, 3),
    ("end", 3, 2), (4, 0, 0), ("far", 3, 3), ("near", 3, 2), (3, 1, 0), (1, 3, 0), ("use", 3, 1), (3, 0, 2),
    (3, 0, 3), ("near", 3, 3), (3, 1, 2), (3, 1, 1), (1, 3, 1), (2, 2, 1), ("end", 3, 3), (3, 2, 0),
    (5, 0, 0), (2, 2, 2), ("use", 3, 2), (2, 2, 3), (4, 0, 2), (4, 0, 1), (2, 3, 0), (2, 3, 1), (1, 3, 2),
    (4, 1, 0), (3, 1, 3), (3, 2, 1), ("use", 3, 3), (4, 0, 3), (3, 2, 2), (1, 3, 3), (5, 0, 3), (3, 2, 3),
    (5, 0, 1), (4, 1, 1), (2, 3, 2), (4, 2, 0), (2, 3, 3), (3, 3, 1), (3, 3, 0), (4, 1, 2), (4, 3, 0),
    (4, 2, 3), (4, 1, 3), (4, 2, 2), (5, 1, 2), (3, 3, 2), (4, 3, 1), (5, 0, 2), (5, 2, 2), (5, 1, 0),
    (5, 2, 3), (5, 2, 0), (5, 1, 1), (4, 2, 1), (3, 3, 3), (4, 3, 2), (5, 1, 3), (5, 2, 1), (4, 3, 3),
)


def direct(s):
    return DIRECT[s]


def kernel(
    n, tok_ref, gain_ref, wg_ref, wu_ref, wd_ref, outv,
    tokv, tokp, normed, bw, bd, acc, hidden, part, r1, sbuf, rz, sx, r2,
    loc_sem, zsend, zrecv, dsend, drecv, ysend, yrecv, vsend, vrecv, tsend, trecv,
    psend, precv, wsend, wrecv, xsend, xrecv, asend, arecv, qsend, qrecv,
):
    z = lax.axis_index("fs")
    y = lax.axis_index("rep")
    t = lax.axis_index("tp")
    c = lax.rem(t, 2)
    tokens, width = tok_ref.shape
    depth, units = wg_ref.shape
    cols = wd_ref.shape[1]
    spans = spans_of(cols)
    half_k, half_t, quarter = depth // 2, tokens // 2, tokens // 4
    sub_k = half_k // SUBS
    most = (units - MID) // 2
    e = lax.rem(z, 2)
    hi = z // 2
    inner = e != hi
    near = z + 1 - 2 * e
    third = 2 - hi
    fourth = 3 - 3 * hi
    pair = {"fs": near}
    has_mid = inner
    mine = pl.multiple_of(e * (most + MID), MID)
    first_unit = pl.multiple_of(e * jnp.where(has_mid, most, most + MID), MID)
    mate = {"tp": t + 1 - 2 * c}
    across = {"tp": lax.rem(t + 2, 4)}
    row = t // 2
    peer = {"rep": 1 - y}

    barrier = pltpu.get_barrier_semaphore()

    around = ({"fs": lax.rem(z + 1, n)}, {"fs": lax.rem(z + n - 1, n)})
    others = tuple({"tp": lax.rem(t + d, 4)} for d in (1, 2, 3))
    for one in around + others + (peer,):
        pl.semaphore_signal(barrier, 1, device_id=one, device_id_type=MESH)
    tok_copy = pltpu.make_async_copy(tok_ref, tokv, loc_sem.at[3])
    tok_copy.start()
    pl.semaphore_wait(barrier, 6)

    def token_move(quart, to, sem, first):
        at = pl.ds(pl.multiple_of(quart * quarter, quarter), quarter)
        return pltpu.make_async_remote_copy(
            src_ref=(tok_ref if first else tokp).at[at],
            dst_ref=tokp.at[at],
            send_sem=tsend.at[sem],
            recv_sem=trecv.at[quart],
            device_id=to,
            device_id_type=MESH,
        )

    def start_of(r, way):
        if r == 1:
            return most, MID
        side = way if r == 0 else 1 - way
        return pl.multiple_of(side * (most + MID), MID), most

    def side_of(r, way):
        return way if r == 0 else 1 - way

    def kept(r, way):
        return inner if r == 1 else side_of(r, way) == e

    def passes(r, way):
        q = side_of(r, way)
        return jnp.logical_or(
            jnp.logical_and(way == 0, z > q), jnp.logical_and(way == 1, z < n - 2 + q))

    def arrives(r, way):
        q = side_of(r, way)
        return jnp.logical_or(
            jnp.logical_and(way == 0, z >= q), jnp.logical_and(way == 1, z < n - 1 + q))

    def pieces(r):
        return range(1 if r == 1 else SUBS)

    def rows_of(r, s, who):
        if r == 1:
            return pl.ds(pl.multiple_of(who * half_k, half_k), half_k)
        return pl.ds(pl.multiple_of(who * half_k + s * sub_k, sub_k), sub_k)

    def along(u, blk, r, s, way, own=None):
        start, size = start_of(r, way)
        at = (rows_of(r, s, y), pl.ds(start, size))
        return pltpu.make_async_remote_copy(
            src_ref=bw.at[(u, blk) + at] if own is None else own.at[at],
            dst_ref=bw.at[(u, blk) + at],
            send_sem=zsend.at[blk, way],
            recv_sem=zrecv.at[u, blk, (0, SUBS, SUBS + 1)[r] + s],
            device_id={"fs": z - 1 + 2 * way},
            device_id_type=MESH,
        )

    def swap(u, blk, i, s, who):
        start, size = ((mine, most), (most, MID))[i]
        place = bw.at[u, blk, rows_of(i, s, who), pl.ds(start, size)]
        return pltpu.make_async_remote_copy(
            src_ref=place,
            dst_ref=place,
            send_sem=ysend.at[blk],
            recv_sem=yrecv.at[u, blk],
            device_id=peer,
            device_id_type=MESH,
        )

    def d_rows(start, size, who):
        return pl.ds(pl.multiple_of(start + who * (size // 2), 64), size // 2)

    def d_along(blk, i, span, r, way, own=False):
        start, size = start_of(r, way)
        at = (d_rows(start, size, y), pl.ds(*span))
        return pltpu.make_async_remote_copy(
            src_ref=wd_ref.at[at] if own else bd.at[(blk,) + at],
            dst_ref=bd.at[(blk,) + at],
            send_sem=dsend.at[blk, way],
            recv_sem=drecv.at[blk, i, r],
            device_id={"fs": z - 1 + 2 * way},
            device_id_type=MESH,
        )

    def d_swap(blk, i, span, p, who):
        start, size = ((mine, most), (most, MID))[p]
        place = bd.at[blk, d_rows(start, size, who), pl.ds(*span)]
        return pltpu.make_async_remote_copy(
            src_ref=place,
            dst_ref=place,
            send_sem=vsend.at[blk],
            recv_sem=vrecv.at[blk, i],
            device_id=peer,
            device_id_type=MESH,
        )

    def own_pieces(way, body):
        for u, own in ((0, wg_ref), (1, wu_ref)):
            for r in range(3):
                @pl.when(passes(r, way))
                def _():
                    for s in pieces(r):
                        body(along(u, z, r, s, way, own))

    def own_d_pieces(way, body):
        for i, span in enumerate(spans):
            for r in range(3):
                pl.when(passes(r, way))(lambda: body(d_along(z, i, span, r, way, True)))

    go = lambda copy: copy.start()
    ZERO, ONE = jnp.int32(0), jnp.int32(1)
    inward, outward = 1 - hi, hi
    @pl.when(inner)
    def _():
        own_pieces(inward, go)
        token_move(t, pair, 0, True).start()
        own_pieces(outward, go)

    @pl.when(jnp.logical_not(inner))
    def _():
        token_move(t, pair, 0, True).start()
        own_pieces(inward, go)
        own_d_pieces(inward, go)

    locals_ = [
        pltpu.make_async_copy(wg_ref, bw.at[0, z], loc_sem.at[0]),
        pltpu.make_async_copy(wu_ref, bw.at[1, z], loc_sem.at[1]),
        pltpu.make_async_copy(wd_ref, bd.at[z], loc_sem.at[2]),
    ]
    for copy in locals_:
        copy.start()

    step = 64

    def norm(src, base):
        @pl.loop(0, tokens // step)
        def _(i):
            at = pl.ds(pl.multiple_of(i * step, step), step)
            to = pl.ds(pl.multiple_of(base + i * step, step), step)
            wide = src[at, :].astype(F32)
            scale = lax.rsqrt(jnp.mean(wide * wide, axis=-1, keepdims=True) + 1e-06)
            normed[to, :] = (wide * scale * gain_ref[...]).astype(BF16)

    def by_size(body):
        pl.when(has_mid)(lambda: body(most + MID))
        pl.when(jnp.logical_not(has_mid))(lambda: body(most))

    def add_dot(u, blk, first=False, last=False, start=0, rows=None):
        rows = depth if rows is None else rows

        def piece(size):
            to = pl.ds(0, size)

            @pl.loop(0, 4)
            def _(i):
                at = pl.ds(pl.multiple_of(i * half_t, half_t), half_t)
                left = normed[at, pl.ds(pl.multiple_of(blk * depth + start, rows), rows)]
                right = bw[u, blk, pl.ds(pl.multiple_of(start, rows), rows), pl.ds(first_unit, size)]
                value = jnp.dot(left, right, preferred_element_type=F32)
                if first:
                    acc[u, at, to] = value
                elif last:
                    hidden[at, to] = (acc[0, at, to] * (acc[1, at, to] + value)).astype(BF16)
                else:
                    acc[u, at, to] = acc[u, at, to] + value

        by_size(piece)

    def activate():
        def piece(size):
            to = pl.ds(0, size)

            @pl.loop(0, 2 * tokens // step)
            def _(i):
                at = pl.ds(pl.multiple_of(i * step, step), step)
                value = acc[0, at, to]
                acc[0, at, to] = value / (1.0 + jnp.exp(-value))

        by_size(piece)

    def place(blk, span, start, size):
        return (
            pl.ds(pl.multiple_of(start, size), size),
            pl.ds(pl.multiple_of(blk * cols + span[0], 128), span[1]),
        )

    def remote(src, dst, sems, at, to):
        return pltpu.make_async_remote_copy(
            src, dst, sems[0].at[at[0]], sems[1].at[at], device_id=to, device_id_type=MESH)

    def to_mate(blk, i, span):
        return remote(part.at[blk, 1, :, :, :, pl.ds(*span)], r1.at[blk, :, :, :, pl.ds(*span)], (psend, precv), (blk, i), mate)

    def line_all(blk, i, span):
        return remote(sbuf.at[blk, 1, :, :, pl.ds(*span)], rz.at[blk, :, :, pl.ds(*span)], (wsend, wrecv), (blk, i), pair)

    def line_one(blk, i, span):
        return remote(sx.at[blk, 1, :, pl.ds(*span)], rz.at[blk, 0, :, pl.ds(*span)], (wsend, wrecv), (blk, i), pair)

    def cross_all(blk, i, span):
        return remote(sx.at[blk, :, :, pl.ds(*span)], r2.at[blk, :, :, pl.ds(*span)], (xsend, xrecv), (blk, i), across)

    def cross_one(blk, i, span):
        return remote(sbuf.at[blk, :, 1 - row, :, pl.ds(*span)], r2.at[blk, :, :, pl.ds(*span)], (xsend, xrecv), (blk, i), across)

    def share(blk, i, span, who):
        at = outv.at[place(blk, span, c * half_t + who * quarter, quarter)]
        return remote(at, at, (asend, arecv), (blk, i), across)

    def give(blk, i, span, who):
        at = outv.at[place(blk, span, who * half_t, half_t)]
        return remote(at, at, (qsend, qrecv), (blk, i), mate)

    def make_part(blk, i, span):
        def fill(size, side):
            @pl.loop(0, 2)
            def _(which):
                whose = c + side - 2 * c * side
                at = pl.ds(pl.multiple_of(which * tokens + whose * half_t, half_t), half_t)
                value = jnp.dot(
                    hidden[at, pl.ds(0, size)], bd[blk, pl.ds(first_unit, size), pl.ds(*span)],
                    preferred_element_type=F32)
                part[blk, side, which, :, :, pl.ds(*span)] = value.astype(BF16).reshape(2, quarter, span[1])

        by_size(lambda size: fill(size, 1))
        to_mate(blk, i, span).start()
        by_size(lambda size: fill(size, 0))

    def sum_mate(blk, i, span):
        to_mate(blk, i, span).wait_recv()
        at = pl.ds(*span)
        sbuf[blk, :, :, :, at] = (part[blk, 0, :, :, :, at].astype(F32) + r1[blk, :, :, :, at].astype(F32)).astype(BF16)

    def direct_1(blk, i, span):
        sum_mate(blk, i, span)
        line_all(blk, i, span).start()

    def direct_2(blk, i, span):
        line_all(blk, i, span).wait_recv()
        at = pl.ds(*span)
        sx[blk, :, :, at] = (sbuf[blk, 0, :, :, at].astype(F32) + rz[blk, :, :, at].astype(F32)).astype(BF16)
        cross_all(blk, i, span).start()

    def direct_3(blk, i, span):
        cross_all(blk, i, span).wait_recv()
        at = pl.ds(*span)
        value = (sx[blk, :, :, at].astype(F32) + r2[blk, :, :, at].astype(F32)).astype(BF16)
        outv[place(blk, span, c * half_t, half_t)] = value.reshape(half_t, span[1])
        give(blk, i, span, c).start()

    def split_1(blk, i, span):
        sum_mate(blk, i, span)
        cross_one(blk, i, span).start()

    def split_2(blk, i, span):
        cross_one(blk, i, span).wait_recv()
        at = pl.ds(*span)
        sx[blk, :, :, at] = (sbuf[blk, :, row, :, at].astype(F32) + r2[blk, :, :, at].astype(F32)).astype(BF16)
        line_one(blk, i, span).start()

    def split_3(blk, i, span):
        line_one(blk, i, span).wait_recv()
        at = pl.ds(*span)
        outv[place(blk, span, c * half_t + row * quarter, quarter)] = (
            sx[blk, 0, :, at].astype(F32) + rz[blk, 0, :, at].astype(F32)).astype(BF16)
        share(blk, i, span, row).start()

    def split_4(blk, i, span):
        share(blk, i, span, 1 - row).wait_recv()
        give(blk, i, span, c).start()

    def store(blk, i, span):
        give(blk, i, span, 1 - c).wait_recv()

    stages = ((split_1, split_2, split_3, split_4, store), (direct_1, direct_2, direct_3, store))

    def way_of(blk):
        return jnp.where(blk < z, ONE, ZERO)

    def arrive(u, blk, rs=(0, 1, 2)):
        way = way_of(blk)
        for r in rs:
            @pl.when(arrives(r, way))
            def _():
                for s in pieces(r):
                    along(u, blk, r, s, way).wait_recv()
                    pl.when(passes(r, way))(lambda: along(u, blk, r, s, way).start())
                    pl.when(kept(r, way))(lambda: swap(u, blk, int(r == 1), s, y).start())

    def all_received(ref, sem):
        pltpu.make_async_remote_copy(ref, ref, zsend.at[0, 0], sem, device_id=peer, device_id_type=MESH).wait_recv()

    def all_sent(ref, sem):
        pltpu.make_async_remote_copy(ref, ref, sem, zrecv.at[0, 0, 0], device_id=peer, device_id_type=MESH).wait_send()

    def swapped(u, blk):
        rows = pl.ds(pl.multiple_of((1 - y) * half_k, half_k), half_k)
        by_size(lambda size: all_received(bw.at[u, blk, rows, pl.ds(first_unit, size)], yrecv.at[u, blk]))

    def d_arrive(blk, i, span, rs=(0, 1, 2)):
        way = way_of(blk)
        for r in rs:
            @pl.when(arrives(r, way))
            def _():
                d_along(blk, i, span, r, way).wait_recv()
                pl.when(passes(r, way))(lambda: d_along(blk, i, span, r, way).start())
                pl.when(kept(r, way))(lambda: d_swap(blk, i, span, int(r == 1), y).start())

    def d_swapped(blk, i, span):
        by_size(lambda size: all_received(bd.at[blk, pl.ds(0, size // 2), pl.ds(*span)], vrecv.at[blk, i]))

    def use(u, blk, last=False):
        if last:
            add_dot(u, blk, start=y * half_k, rows=half_k)
            swapped(u, blk)
            add_dot(u, blk, last=True, start=(1 - y) * half_k, rows=half_k)
        else:
            swapped(u, blk)
            add_dot(u, blk)

    zero_in = jnp.where(inner, ZERO, ONE)
    events = (
        (ZERO, jnp.where(inner, third, near)),
        (zero_in, near),
        (1 - zero_in, third),
        (ONE, jnp.where(inner, near, third)),
        (ZERO, fourth),
        (ONE, fourth),
    )

    tok_copy.wait()
    norm(tokv, 0)
    for copy in locals_:
        copy.wait()
    pl.when(inner)(lambda: arrive(*events[0]))
    token_move(t, pair, 0, True).wait_recv()
    for i, one in enumerate(others):
        token_move(t, one, 1 + i, False).start()
    outer = jnp.logical_not(inner)
    pl.when(outer)(lambda: arrive(*events[0]))
    arrive(*events[1])
    arrive(*events[2])
    for d in (1, 2, 3):
        token_move(lax.rem(t + d, 4), mate, 0, False).wait_recv()
    norm(tokp, tokens)
    pl.when(inner)(lambda: arrive(*events[3], rs=(0,)))
    for u in (0, 1):
        add_dot(u, z, first=True)
    pl.when(inner)(lambda: arrive(*events[4], rs=(0, 1)))
    pl.when(outer)(lambda: arrive(*events[3]))
    use(*events[0])

    @pl.when(inner)
    def _():
        arrive(*events[3], rs=(1, 2))
        own_d_pieces(inward, go)

    use(*events[1])
    use(*events[2])
    pl.when(inner)(lambda: arrive(*events[4], rs=(2,)))
    pl.when(outer)(lambda: arrive(*events[4]))
    use(*events[3])

    @pl.when(inner)
    def _():
        arrive(*events[5], rs=(0,))

    use(*events[4])

    @pl.when(inner)
    def _():
        arrive(*events[5], rs=(1,))
        own_d_pieces(outward, go)

    activate()
    pl.when(outer)(lambda: arrive(*events[5]))

    @pl.when(inner)
    def _():
        arrive(*events[5], rs=(2,))
        for i, span in enumerate(spans):
            d_arrive(near, i, span)
    blocks = (z, near, third, fourth)
    for kind, s, i in ORDER:
        blk, span = blocks[s], spans[i]
        if kind == "last":
            use(*events[5], last=True)
        elif kind == "far":
            pl.when(inner)(lambda: d_arrive(blk, i, span, (0, 1)))
        elif kind == "near":
            pl.when(inner)(lambda: d_arrive(blk, i, span, (2,)))
        elif kind == "end":
            pl.when(outer)(lambda: d_arrive(blk, i, span))
        elif kind == "use":
            if s > 0:
                d_swapped(blk, i, span)
            make_part(blk, i, span)
        else:
            stages[direct(s)][kind - 1](blk, i, span)

    token_move(t, pair, 0, True).wait_send()
    for i, one in enumerate(others):
        token_move(t, one, 1 + i, False).wait_send()

    def sent_along(blk, way):
        def wait(size):
            all_sent(bw.at[:, blk, pl.ds(0, half_k), pl.ds(0, size)], zsend.at[blk, way])
            all_sent(bd.at[blk, pl.ds(0, size // 2)], dsend.at[blk, way])

        some = jnp.logical_and(passes(0, way), jnp.logical_not(passes(2, way)))
        pl.when(passes(2, way))(lambda: wait(units))
        pl.when(jnp.logical_and(some, passes(1, way)))(lambda: wait(most + MID))
        pl.when(jnp.logical_and(some, jnp.logical_not(passes(1, way))))(lambda: wait(most))

    def sent_swap(blk):
        def wait(size):
            all_sent(bw.at[:, blk, pl.ds(0, half_k), pl.ds(0, size)], ysend.at[blk])
            all_sent(bd.at[blk, pl.ds(0, size // 2)], vsend.at[blk])

        by_size(wait)

    sent_along(z, ZERO)
    sent_along(z, ONE)
    whole = (0, cols)
    for s, blk in enumerate(blocks):
        def settle():
            sent_along(blk, way_of(blk))
            sent_swap(blk)

        if s > 0:
            settle()
        all_sent(part.at[blk, 1], psend.at[blk])
        if direct(s):
            all_sent(sbuf.at[blk, 1], wsend.at[blk])
            all_sent(sx.at[blk], xsend.at[blk])
        else:
            all_sent(sbuf.at[blk, :, 0], xsend.at[blk])
            all_sent(sx.at[blk, 1], wsend.at[blk])
            all_sent(outv.at[place(blk, whole, 0, quarter)], asend.at[blk])
        all_sent(outv.at[place(blk, whole, 0, half_t)], qsend.at[blk])


def fused(n, tokens, norm_gain, gate_weight, up_weight, down_weight):
    rows, width = tokens.shape
    depth, units = gate_weight.shape
    cols = down_weight.shape[1]
    held = (units + MID) // 2
    dma = pltpu.SemaphoreType.DMA
    quarter = rows // 4
    hbm = pl.BlockSpec(memory_space=pl.ANY)
    vmem = pl.BlockSpec(memory_space=pltpu.VMEM)
    return pl.pallas_call(
        functools.partial(kernel, n),
        out_shape=pltpu.VMEM((rows, width), BF16),
        in_specs=[hbm, vmem, hbm, hbm, hbm],
        out_specs=vmem,
        scratch_shapes=[
            pltpu.VMEM((rows, width), BF16),
            pltpu.VMEM((rows, width), BF16),
            pltpu.VMEM((2 * rows, width), BF16),
            pltpu.VMEM((2, n, depth, units), BF16),
            pltpu.VMEM((n, units, cols), BF16),
            pltpu.VMEM((2, 2 * rows, held), F32),
            pltpu.VMEM((2 * rows, held), BF16),
            pltpu.VMEM((n, 2, 2, 2, quarter, cols), BF16),
            pltpu.VMEM((n, 2, 2, quarter, cols), BF16),
            pltpu.VMEM((n, 2, 2, quarter, cols), BF16),
            pltpu.VMEM((n, 2, quarter, cols), BF16),
            pltpu.VMEM((n, 2, quarter, cols), BF16),
            pltpu.VMEM((n, 2, quarter, cols), BF16),
            dma((4,)),
            dma((n, 2)),
            dma((2, n, 2 * SUBS + 1)),
            dma((n, 2)),
            dma((n, MOST_CUTS, 3)),
            dma((n,)),
            dma((2, n)),
            dma((n,)),
            dma((n, MOST_CUTS)),
            dma((4,)),
            dma((4,)),
        ] + 5 * [dma((n,)), dma((n, MOST_CUTS))],
        compiler_params=pltpu.CompilerParams(
            collective_id=0, has_side_effects=True, vmem_limit_bytes=60 * 2**20
        ),
    )(tokens, norm_gain.reshape(1, width), gate_weight, up_weight, down_weight)


def solution(mesh):
    n = mesh.shape["fs"]
    small = mesh.shape["rep"] == 2 and mesh.shape["tp"] == 4 and n == 4
    body = functools.partial(fused, n) if small else plain
    in_specs = (P(("rep", "fs"), None), P(), P("fs", "tp"), P("fs", "tp"), P("tp", "fs"))
    out_specs = P(("rep", "fs"), None)
    return jax.shard_map(
        body, mesh=mesh, in_specs=in_specs, out_specs=out_specs, check_vma=False
    )
```
